32 devices in a mesh: grp: 2 (over y), sp: 4 (over z), tp: 4 (over x, core).
Axes of the slice: x: 2, y: 2, z: 4, core: 2. Of those that a mesh axis runs over, the one named last changes fastest.
Arguments:
- queries: bfloat16 [4096, 2048], P(('grp', 'sp'), 'tp'), parts along dimension 0, may hold values from -64 to 64
- key_heads: bfloat16 [4096, 4, 64], P(('grp', 'sp'), 'tp'), parts along dimension 0, may hold values from -64 to 64
- value_heads: bfloat16 [4096, 4, 64], P(('grp', 'sp'), 'tp'), parts along dimension 0, may hold values from -6 to 6
- sink_logit: float32 [32], P('tp'), may hold values from 3 to 6
- out_weight: bfloat16 [2048, 2048], P('tp'), may hold values from -0.75 to 0.75
- residual: bfloat16 [4096, 2048], P(('grp', 'sp', 'tp')), parts along dimension 0, may hold values from -6 to 6
- norm_gain: float32 [2048], replicated, may hold values from 0.1 to 1.9
- expert_ids: int32 [4096, 2], P(('grp', 'sp', 'tp')), parts along dimension 0, may hold values from 0 to 15, all different within a row; in each aligned block of 128 rows (0 to 127, 128 to 255, ...) at most 32 rows name the same one
- route_weights: float32 [4096, 2], P(('grp', 'sp', 'tp')), parts along dimension 0, may hold values from 0.1 to 1
- gate_weight: bfloat16 [16, 2048, 512], P(('sp', 'tp')), may hold values from -0.125 to 0.125
- up_weight: bfloat16 [16, 2048, 512], P(('sp', 'tp')), may hold values from -0.125 to 0.125
- down_weight: bfloat16 [16, 512, 2048], P(('sp', 'tp')), may hold values from -0.5 to 0.5
Outputs:
- mixed: bfloat16 [4096, 2048], P(('grp', 'sp', 'tp')), parts along dimension 0
The draws below stay inside these ranges and needn't reach their ends.
There are 2 independent parts, one for each index of `grp`. The reference program is written for one: setup_inputs(seed, part) draws one part's arguments, and reference() takes and returns one part's arrays. A program takes and returns all parts, laid end to end along the dimension named above; an argument that names none is the same for every part. Nothing has to cross between parts.
Inputs may be any that keep to these rules, and one draw needn't show every extreme that they name: `expert_ids`: each row names 2 different experts. In the rows of one device (aligned blocks of 128 rows) no expert is named more than 32 times, and in some blocks one expert is named exactly 32 times.
All inputs are finite; a program needn't handle non-finite values.
Results may differ from the reference program's by a relative error of at most 0.014.
Values may be sent and summed in bfloat16 or wider, within the bound.
A program may use at most 64 MiB of HBM per device.

```python
import math
import jax
import jax.numpy as jnp
import numpy as np
from jax import lax

D = 2048
QH = 32
KVH = 4
HEAD_SIZE = 64
WINDOW = 128
FF = 512
TOP_K = 2
TOK_DEV = 128
TOKENS = 2048
EXPERTS = 16
CAP = 32


def draw_queries(key, part):
    drawn = jnp.clip(jax.random.normal(jax.random.fold_in(key, 5), (TOKENS, QH * HEAD_SIZE), jnp.float32), -6.0, 6.0)
    return drawn.astype(jnp.bfloat16)


def draw_key_heads(key, part):
    drawn = jnp.clip(jax.random.normal(jax.random.fold_in(key, 6), (TOKENS, KVH, HEAD_SIZE), jnp.float32), -6.0, 6.0)
    return drawn.astype(jnp.bfloat16)


def steps_of(own_key, dims, pieces, least, largest):
    level, own = 1.0, jax.random.fold_in(own_key, 6)
    for position, parts in pieces:
        steps = jnp.exp(jax.random.uniform(jax.random.fold_in(own, position), (parts,), jnp.float32, least / len(pieces), largest / len(pieces)))
        level = level * jnp.repeat(steps, dims[position] // parts).reshape([-1 if axis == position else 1 for axis in range(len(dims))])
    return level


def assign_block(own_key, own, number, rows, amount, top, limit, lean):
    ranking = jax.random.permutation(own_key, amount)
    crowded, ordinary = portions_of(amount, rows * top, limit, lean, True), portions_of(amount, rows * top, limit, lean, False)
    places = jnp.arange(amount)

    def named(sizes, turn):
        used = int((sizes > 0).sum())
        fixed = max(1, used // 4)
        shifted = fixed + (places - fixed + turn * (used - fixed)) % max(1, amount - fixed)
        return jnp.zeros((amount,), jnp.int32).at[ranking[jnp.where(places < fixed, places, shifted)]].set(jnp.asarray(sizes, jnp.int32))

    sizes = jnp.where(number % 4 == 0, named(crowded, number // 4), named(ordinary, number - number // 4 - 1))
    mixed = jax.random.permutation(jax.random.fold_in(own, 3), amount)
    giver, receiver = mixed[0:amount // 2 * 2:2], mixed[1:amount // 2 * 2:2]
    room = jnp.minimum(sizes[giver] - 1, limit - sizes[receiver]) // 2
    room = jnp.where((giver == ranking[0]) | (receiver == ranking[0]) | (sizes[receiver] == 0), 0, jnp.maximum(room, 0))
    shifted = jax.random.randint(jax.random.fold_in(own, 4), (amount // 2,), 0, 1 << 20) % (room + 1)
    sizes = sizes.at[giver].add(-shifted).at[receiver].add(shifted)
    members = jnp.searchsorted(jnp.cumsum(sizes), jnp.arange(rows * top), side="right").astype(jnp.int32)
    table = members.reshape(top, rows).T
    table = table[jax.random.permutation(jax.random.fold_in(own, 1), rows)]
    turn = jax.random.randint(jax.random.fold_in(own, 2), (rows, 1), 0, top)
    return jnp.take_along_axis(table, (jnp.arange(top)[None, :] + turn) % top, axis=1)


def portions_of(amount, total, limit, skew, full):
    loads = [(1 << 20) // math.isqrt(grade ** skew) + 1 for grade in range(1, amount + 1)]
    largest = limit if full else min(limit, max(-(-total // amount), total * loads[0] // sum(loads)))
    least = 1 if total - largest >= amount - 1 else 0
    holding, rest = [largest] + [least] * (amount - 1), total - largest - least * (amount - 1)
    while rest > 0:
        free = [i for i in range(1, amount) if holding[i] < largest] or [i for i in range(1, amount) if holding[i] < limit]
        whole, left = sum([loads[i] for i in free]), rest
        for i in free:
            extra = min(limit - holding[i], max(1, left * loads[i] // whole), rest)
            holding[i] = holding[i] + extra
            rest = rest - extra
    return np.array(holding)


def normal_values(rng, dims, deviation, limit, pieces=(), kind=jnp.bfloat16):
    gain = steps_of(rng, dims, pieces, -0.22, 0.18) if pieces else 1.0
    result = jax.random.normal(rng, dims, jnp.float32) * deviation * gain
    return jnp.minimum(jnp.maximum(result, -limit), limit).astype(kind)


def setup_inputs(seed: int = 0, part: int = 0) -> dict:
    key_list = jax.random.split(jax.random.key(seed), 13)
    own_keys = jax.random.split(jax.random.fold_in(key_list[12], part), 13)
    queries = draw_queries(jax.random.fold_in(jax.random.fold_in(key_list[12], part), 71), part)
    key_heads = draw_key_heads(jax.random.fold_in(jax.random.fold_in(key_list[12], part), 71), part)
    value_heads = normal_values(own_keys[2], (TOKENS, KVH, HEAD_SIZE), 1.0, 6.0, ((0, 4), (1, 4)))
    sink_logit = jnp.clip(3.0 + 3.0 * jax.random.uniform(key_list[3], (QH,), jnp.float32) ** steps_of(key_list[3], (QH,), ((0, 4),), -0.2, 0.2), 3.0, 6.0)
    out_weight = normal_values(key_list[4], (QH * HEAD_SIZE, D), (QH * HEAD_SIZE // 32) ** -0.5, 0.75, ((0, 4),))
    residual = normal_values(own_keys[5], (TOKENS, D), 1.0, 6.0, ((0, 16),))
    norm_gain = jnp.clip(1.0 + 0.18 * jax.random.normal(key_list[6], (D,), jnp.float32), 0.1, 1.9)
    expert_ids_keys = jax.random.split(jax.random.fold_in(own_keys[7], 1), TOKENS // TOK_DEV)
    expert_ids_turns = jax.random.permutation(jax.random.fold_in(own_keys[7], 3), TOKENS // TOK_DEV)
    expert_ids = jax.vmap(lambda own, number: assign_block(jax.random.fold_in(own_keys[7], 2), own, number, TOK_DEV, EXPERTS, TOP_K, CAP, 1))(expert_ids_keys, expert_ids_turns).reshape((TOKENS, TOP_K))
    route_weights = jnp.clip(jnp.exp(math.log(1.0) - 2.3025851 * jax.random.uniform(own_keys[8], (TOKENS, TOP_K), jnp.float32) ** steps_of(own_keys[8], (TOKENS, TOP_K), ((0, 16),), -0.2, 0.2)), 0.1, 1.0)
    gate_weight = normal_values(key_list[9], (EXPERTS, D, FF), D ** -0.5, 0.125, ((0, 16),))
    up_weight = normal_values(key_list[10], (EXPERTS, D, FF), D ** -0.5, 0.125, ((0, 16),))
    down_weight = normal_values(key_list[11], (EXPERTS, FF, D), (FF // 4) ** -0.5, 0.5, ((0, 16),))
    return dict(queries=queries, key_heads=key_heads, value_heads=value_heads, sink_logit=sink_logit, out_weight=out_weight, residual=residual, norm_gain=norm_gain, expert_ids=expert_ids, route_weights=route_weights, gate_weight=gate_weight, up_weight=up_weight, down_weight=down_weight)


EPS = 1e-06

def attention(queries, key_heads, value_heads, sink_logit):
    group_size = QH // KVH
    count_of_blocks = TOKENS // WINDOW
    query_blocks = queries.reshape(count_of_blocks, WINDOW, KVH, group_size, HEAD_SIZE)
    key_blocks = key_heads.reshape(count_of_blocks, WINDOW, KVH, HEAD_SIZE)
    value_blocks = value_heads.reshape(count_of_blocks, WINDOW, KVH, HEAD_SIZE)
    blank = jnp.zeros((1, WINDOW, KVH, HEAD_SIZE), key_heads.dtype)
    key_span = jnp.concatenate([jnp.concatenate([blank, key_blocks[:-1]], 0), key_blocks], 1)
    value_span = jnp.concatenate([jnp.concatenate([blank, value_blocks[:-1]], 0), value_blocks], 1)
    query_pos = jnp.arange(WINDOW, dtype=jnp.int32)[:, None]
    key_pos = jnp.arange(2 * WINDOW, dtype=jnp.int32)[None, :]
    distance = query_pos + WINDOW - key_pos
    band = (distance >= 0) & (distance < WINDOW)
    key_start = jnp.arange(count_of_blocks, dtype=jnp.int32)[:, None] * WINDOW - WINDOW + key_pos
    allowed = band[None, :, :] & (key_start >= 0)[:, None, :]
    sinks = sink_logit.reshape(KVH, group_size)

    def one_head(packed):
        query_per_head, key_per_head, value_per_head, head_sink = packed
        logit_scores = jnp.einsum('szue,sje->suzj', query_per_head.astype(jnp.float32), key_per_head.astype(jnp.float32)) * HEAD_SIZE ** (-0.5)
        logit_scores = jnp.where(allowed[:, None], logit_scores, -jnp.inf)
        sink_col = head_sink[None, :, None, None]
        row_max = jnp.maximum(lax.optimization_barrier(jnp.max(logit_scores, axis=-1, keepdims=True)), sink_col)
        expd = jnp.exp(logit_scores - row_max)
        row_total = lax.optimization_barrier(jnp.sum(expd, axis=-1, keepdims=True)) + jnp.exp(sink_col - row_max)
        attention_probabilities = (expd / row_total).astype(jnp.bfloat16)
        return jnp.einsum('vjwu,vuo->vwjo', attention_probabilities.astype(jnp.float32), value_per_head.astype(jnp.float32)).astype(jnp.bfloat16)
    outputs = lax.map(one_head, (jnp.moveaxis(query_blocks, 2, 0), jnp.moveaxis(key_span, 2, 0), jnp.moveaxis(value_span, 2, 0), sinks))
    return jnp.moveaxis(outputs, 0, 2).reshape(TOKENS, QH * HEAD_SIZE)

def reference(queries, key_heads, value_heads, sink_logit, out_weight, residual, norm_gain, expert_ids, route_weights, gate_weight, up_weight, down_weight):
    attended = attention(queries, key_heads, value_heads, sink_logit)
    projected = jnp.dot(attended, out_weight, preferred_element_type=jnp.float32)
    stream = (residual.astype(jnp.float32) + projected).astype(jnp.bfloat16)
    wide = stream.astype(jnp.float32)
    normed = (wide * lax.rsqrt(lax.optimization_barrier(jnp.mean(wide * wide, axis=-1, keepdims=True)) + EPS) * norm_gain).astype(jnp.bfloat16)
    device_count = TOKENS // TOK_DEV
    pairs = TOK_DEV * TOP_K
    flat_ids = expert_ids.reshape(device_count, pairs)
    onehot = (flat_ids[:, :, None] == jnp.arange(EXPERTS, dtype=jnp.int32)[None, None, :]).astype(jnp.int32)
    earlier = jnp.cumsum(onehot, axis=1) - onehot
    slot_rank = lax.optimization_barrier(jnp.sum(earlier * onehot, axis=-1))
    flat_slot = (flat_ids * CAP + slot_rank).astype(jnp.int32)
    device_row = jnp.arange(device_count, dtype=jnp.int32)[:, None]
    owner_row = device_row * TOK_DEV + (jnp.arange(pairs, dtype=jnp.int32) // TOP_K)[None, :]
    shares = route_weights / lax.optimization_barrier(jnp.sum(route_weights, axis=-1, keepdims=True))
    token_in_slot = jnp.zeros((device_count, EXPERTS * CAP), jnp.int32).at[device_row, flat_slot].set(owner_row)
    slot_share = jnp.zeros((device_count, EXPERTS * CAP), jnp.float32).at[device_row, flat_slot].set(shares.reshape(device_count, pairs))

    def expert_step(summed, packed):
        w_gate_e, w_up_e, w_down_e, expert = packed
        row_index = lax.dynamic_slice_in_dim(token_in_slot, expert * CAP, CAP, 1).reshape(-1)
        row_share = lax.dynamic_slice_in_dim(slot_share, expert * CAP, CAP, 1).reshape(-1)
        rows = normed[row_index]
        gate = jnp.dot(rows, w_gate_e, preferred_element_type=jnp.float32)
        upward = jnp.dot(rows, w_up_e, preferred_element_type=jnp.float32)
        expert_hidden = (jax.nn.silu(gate) * upward).astype(jnp.bfloat16)
        expert_rows = jnp.dot(expert_hidden, w_down_e, preferred_element_type=jnp.float32).astype(jnp.bfloat16)
        summed = summed.at[row_index].add(row_share[:, None] * expert_rows.astype(jnp.float32))
        return (summed, None)
    start = jnp.zeros((TOKENS, D), jnp.float32)
    summed, _ = lax.scan(expert_step, start, (gate_weight, up_weight, down_weight, jnp.arange(EXPERTS, dtype=jnp.int32)))
    return (stream.astype(jnp.float32) + summed).astype(jnp.bfloat16)
```

```python
import functools

import jax
import jax.numpy as jnp
from jax import lax
from jax.experimental import pallas as pl
from jax.experimental.pallas import tpu as pltpu
from jax.sharding import PartitionSpec as P

WINDOW = 128


EPS = 1e-06

F32 = jnp.float32
BF16 = jnp.bfloat16
MESH = pl.DeviceIdType.MESH
VMEM_BUDGET = 56 * 1024 * 1024


def from_behind(value, axis, steps):
    count = lax.axis_size(axis)
    initial, last = (max(0, -steps), min(count, count - steps))
    return lax.ppermute(value, axis, [(source, source + steps) for source in range(initial, last)])


def dot(a, b, dims=((1,), (0,))):
    return lax.dot_general(a, b, (dims, ((), ())), preferred_element_type=F32)


def attention(queries, key_heads, value_heads, sink_logit):
    rows_sp = queries.shape[0]
    kv_local = key_heads.shape[1]
    head_dim = key_heads.shape[2]
    heads_local = queries.shape[1] // head_dim
    group_size = heads_local // kv_local
    window = WINDOW
    count_of_blocks = rows_sp // window
    edge = jnp.stack([key_heads[rows_sp - window :], value_heads[rows_sp - window :]])
    tail_rows = from_behind(edge, "sp", 1)
    key_blocks = jnp.concatenate([tail_rows[0], key_heads], 0).reshape(
        count_of_blocks + 1, window, kv_local, head_dim
    )
    value_blocks = jnp.concatenate([tail_rows[1], value_heads], 0).reshape(
        count_of_blocks + 1, window, kv_local, head_dim
    )
    key_span = jnp.concatenate([key_blocks[:-1], key_blocks[1:]], 1)
    value_span = jnp.concatenate([value_blocks[:-1], value_blocks[1:]], 1)
    query_pos = jnp.arange(window, dtype=jnp.int32)[:, None]
    key_pos = jnp.arange(2 * window, dtype=jnp.int32)[None, :]
    distance = query_pos + window - key_pos
    band = (distance >= 0) & (distance < window)
    key_start = (
        lax.axis_index("sp") * rows_sp
        + jnp.arange(count_of_blocks, dtype=jnp.int32)[:, None] * window
        - window
        + key_pos
    )
    allowed = band[None, :, :] & (key_start >= 0)[:, None, :]
    query_blocks = queries.reshape(count_of_blocks, window, kv_local, group_size, head_dim)
    logit_scores = jnp.einsum(
        "bqhgd,bkhd->bhgqk", query_blocks, key_span, preferred_element_type=jnp.float32
    ) * head_dim ** (-0.5)
    logit_scores = jnp.where(allowed[:, None, None], logit_scores, -jnp.inf)
    sink_col = sink_logit.reshape(kv_local, group_size)[None, :, :, None, None]
    row_max = jnp.maximum(jnp.max(logit_scores, axis=-1, keepdims=True), sink_col)
    expd = jnp.exp(logit_scores - row_max)
    row_total = jnp.sum(expd, axis=-1, keepdims=True) + jnp.exp(sink_col - row_max)
    attention_probabilities = (expd / row_total).astype(jnp.bfloat16)
    attended = jnp.einsum(
        "bhgqk,bkhd->bqhgd", attention_probabilities, value_span, preferred_element_type=jnp.float32
    ).astype(jnp.bfloat16)
    return attended.reshape(rows_sp, heads_local * head_dim)


def tail_plain(
    attended, out_weight, residual, norm_gain, expert_ids, route_weights,
    gate_weight, up_weight, down_weight,
):
    rows_dev = residual.shape[0]
    width = residual.shape[1]
    projected = lax.psum_scatter(
        jnp.dot(attended, out_weight, preferred_element_type=jnp.float32),
        "tp",
        scatter_dimension=0,
        tiled=True,
    )
    stream = (residual.astype(jnp.float32) + projected).astype(jnp.bfloat16)
    wide = stream.astype(jnp.float32)
    normed = (
        wide * lax.rsqrt(jnp.mean(wide * wide, axis=-1, keepdims=True) + EPS) * norm_gain
    ).astype(jnp.bfloat16)
    sp_count = lax.axis_size("sp")
    tp_count = lax.axis_size("tp")
    experts_total = sp_count * tp_count
    top_k = expert_ids.shape[1]
    capacity = max(2, 2 * top_k * rows_dev // experts_total)
    flat_ids = expert_ids.reshape(-1)
    pairs = flat_ids.shape[0]
    onehot = (flat_ids[:, None] == jnp.arange(experts_total, dtype=jnp.int32)[None, :]).astype(
        jnp.int32
    )
    earlier = jnp.cumsum(onehot, axis=0) - onehot
    slot_rank = jnp.sum(earlier * onehot, axis=1)
    flat_slot = flat_ids * capacity + slot_rank
    owner_row = jnp.arange(pairs, dtype=jnp.int32) // top_k
    token_in_slot = jnp.zeros((experts_total * capacity,), jnp.int32).at[flat_slot].set(owner_row)
    filled = jnp.zeros((experts_total * capacity,), jnp.bool_).at[flat_slot].set(True)
    outbox = jnp.where(filled[:, None], normed[token_in_slot], jnp.zeros((), jnp.bfloat16))
    outbox = outbox.reshape(experts_total, capacity, width)
    arrived = lax.all_to_all(outbox, ("sp", "tp"), split_axis=0, concat_axis=0, tiled=True)
    rows = arrived.reshape(-1, width)
    gate = jnp.dot(rows, gate_weight[0], preferred_element_type=jnp.float32)
    upward = jnp.dot(rows, up_weight[0], preferred_element_type=jnp.float32)
    expert_hidden = (jax.nn.silu(gate) * upward).astype(jnp.bfloat16)
    expert_rows = jnp.dot(expert_hidden, down_weight[0], preferred_element_type=jnp.float32).astype(
        jnp.bfloat16
    )
    results = expert_rows.reshape(arrived.shape)
    returned = lax.all_to_all(results, ("sp", "tp"), split_axis=0, concat_axis=0, tiled=True)
    picked_rows = returned.reshape(experts_total * capacity, width)[flat_slot].reshape(
        rows_dev, top_k, width
    )
    shares = route_weights / jnp.sum(route_weights, axis=-1, keepdims=True)
    combined = jnp.sum(shares[:, :, None] * picked_rows.astype(jnp.float32), axis=1)
    return (wide + combined).astype(jnp.bfloat16)


def routing(ids, weights, experts, capacity):
    rows, top_k = ids.shape
    expert = lax.broadcasted_iota(jnp.int32, (rows, experts), 1)
    total = jnp.sum(weights, axis=1, keepdims=True)
    member = jnp.zeros((rows, experts), F32)
    share = jnp.zeros((rows, experts), F32)
    for k in range(top_k):
        hit = (ids[:, k : k + 1] == expert).astype(F32)
        member = member + hit
        share = share + hit * (weights[:, k : k + 1] / total)
    before = (
        lax.broadcasted_iota(jnp.int32, (rows, rows), 0)
        > lax.broadcasted_iota(jnp.int32, (rows, rows), 1)
    ).astype(BF16)
    rank = dot(before, member.astype(BF16))
    rank = jnp.where(member > 0, rank, -1.0)
    slots = experts * capacity
    spread = (
        lax.broadcasted_iota(jnp.int32, (experts, slots), 1) // capacity
        == lax.broadcasted_iota(jnp.int32, (experts, slots), 0)
    ).astype(BF16)
    rank_slot = dot(rank.astype(BF16), spread)
    place = lax.broadcasted_iota(jnp.int32, (rows, slots), 1) % capacity
    taken = rank_slot == place.astype(F32)
    high = share.astype(BF16)
    low = (share - high.astype(F32)).astype(BF16)
    one = jnp.where(taken, 1.0, 0.0)
    return (
        one.astype(BF16),
        (one * dot(high, spread)).astype(BF16),
        (one * dot(low, spread)).astype(BF16),
    )


def tail_kernel(
    sizes,
    attended, out_w_hbm, residual, gain, ids, weights, gate_hbm, up_hbm, down_hbm,
    out,
    out_w, gate_w, up_w, down_w,
    pair_out, pair_in, far_out, far_in,
    stream, normed, slots, share_hi, share_lo,
    outbox, arrived, results, returned,
    load_sem, pair_send, pair_recv, far_send, far_recv,
    go_send, go_recv, back_send, back_recv,
):
    sp_count, tp_count, pieces, capacity = sizes
    experts = sp_count * tp_count
    chips = tp_count // 2
    z, t = lax.axis_index("sp"), lax.axis_index("tp")
    me = z * tp_count + t
    x, core = t // 2, t % 2
    other = 1 - core
    rows, width = residual.shape
    piece = width // pieces

    def where(e):
        return {"sp": e // tp_count, "tp": e % tp_count}

    loads = [
        pltpu.make_async_copy(src, dst, load_sem.at[i])
        for i, (src, dst) in enumerate(
            ((out_w_hbm, out_w), (gate_hbm.at[0], gate_w), (up_hbm.at[0], up_w), (down_hbm.at[0], down_w))
        )
    ]
    for load in loads:
        load.start()

    barrier = pltpu.get_barrier_semaphore()

    def greet(k, carry):
        pl.semaphore_signal(
            barrier, inc=1, device_id=where((me + k) % experts), device_id_type=MESH
        )
        return carry

    lax.fori_loop(1, experts, greet, 0)
    slots[...], share_hi[...], share_lo[...] = routing(ids[...], weights[...], experts, capacity)
    loads[0].wait()
    pl.semaphore_wait(barrier, experts - 1)

    def partial(chip, which, q):
        block = attended[pl.ds(pl.multiple_of((chip * 2 + which) * rows, rows), rows), :]
        return dot(block, out_w[:, q * piece : (q + 1) * piece])

    def pair_copy(k, q):
        return pltpu.make_async_remote_copy(
            pair_out.at[k, q], pair_in.at[k, q], pair_send.at[k, q], pair_recv.at[k, q],
            device_id={"tp": x * 2 + other}, device_id_type=MESH,
        )

    def far_copy(k, q):
        return pltpu.make_async_remote_copy(
            far_out.at[k, q], far_in.at[k, q], far_send.at[k, q], far_recv.at[k, q],
            device_id={"tp": ((x + k) % chips) * 2 + core}, device_id_type=MESH,
        )

    order = list(range(1, chips)) + [0]
    for q in range(pieces):
        for k in order:
            pair_out[k, q] = partial((x + k) % chips, other, q).astype(BF16)
            pair_copy(k, q).start()
        for k in range(1, chips):
            mine = partial((x + k) % chips, core, q)
            pair_copy(k, q).wait_recv()
            far_out[k, q] = (mine + pair_in[k, q].astype(F32)).astype(BF16)
            far_copy(k, q).start()
    square = jnp.zeros((rows, 1), F32)
    for q in range(pieces):
        cols = slice(q * piece, (q + 1) * piece)
        total = partial(x, core, q)
        pair_copy(0, q).wait_recv()
        total = total + pair_in[0, q].astype(F32)
        for k in range(1, chips):
            far_copy(k, q).wait_recv()
            total = total + far_in[k, q].astype(F32)
        value = (residual[:, cols].astype(F32) + total).astype(BF16)
        stream[:, cols] = value
        value = value.astype(F32)
        square = square + jnp.sum(value * value, axis=1, keepdims=True)
    scale = lax.rsqrt(square / width + EPS)
    for q in range(pieces):
        cols = slice(q * piece, (q + 1) * piece)
        normed[:, cols] = (stream[:, cols].astype(F32) * scale * gain[:, cols]).astype(BF16)

    def go_copy(to, at):
        return pltpu.make_async_remote_copy(
            outbox.at[to], arrived.at[at], go_send.at[to], go_recv.at[at],
            device_id=where(to), device_id_type=MESH,
        )

    def back_copy(to, at):
        return pltpu.make_async_remote_copy(
            results.at[to], returned.at[at], back_send.at[to], back_recv.at[at],
            device_id=where(to), device_id_type=MESH,
        )

    picks = tp_count * capacity
    for d in range(sp_count):
        layer = range(d * tp_count, (d + 1) * tp_count)
        chosen = dot(slots[:, d * picks : (d + 1) * picks], normed[...], ((0,), (0,))).astype(BF16)
        for i, e in enumerate(layer):
            outbox[e] = chosen[i * capacity : (i + 1) * capacity]

            @pl.when(e != me)
            def _():
                go_copy(e, me).start()

    arrived[me] = outbox[me]
    for load in loads[1:]:
        load.wait()

    def expert(d, carry):
        layer = (z + d) % sp_count
        for i in range(tp_count):
            e = layer * tp_count + i

            @pl.when(e != me)
            def _():
                go_copy(me, e).wait_recv()

        block = arrived[pl.ds(layer * tp_count, tp_count)].reshape(picks, width)
        gated = dot(block, gate_w[...])
        raised = dot(block, up_w[...])
        hidden = (gated / (1.0 + jnp.exp(-gated)) * raised).astype(BF16)
        done = dot(hidden, down_w[...]).astype(BF16)
        results[pl.ds(layer * tp_count, tp_count)] = done.reshape(tp_count, capacity, width)
        for i in range(tp_count):
            e = layer * tp_count + i

            @pl.when(e != me)
            def _():
                back_copy(e, me).start()

        return carry

    lax.fori_loop(0, sp_count, expert, 0)
    returned[me] = results[me]

    def collect(k, carry):
        e = (me + k) % experts
        back_copy(me, e).wait_recv()
        return carry

    lax.fori_loop(1, experts, collect, 0)
    for q in range(pieces):
        cols = slice(q * piece, (q + 1) * piece)
        back = returned[:, :, cols].reshape(experts * capacity, piece)
        mixed = dot(share_hi[...], back) + dot(share_lo[...], back)
        out[:, cols] = (stream[:, cols].astype(F32) + mixed).astype(BF16)

    for q in range(pieces):
        for k in range(chips):
            pair_copy(k, q).wait_send()
            if k:
                far_copy(k, q).wait_send()

    def flush(k, carry):
        e = (me + k) % experts
        go_copy(e, me).wait_send()
        back_copy(e, me).wait_send()
        return carry

    lax.fori_loop(1, experts, flush, 0)


def tail_fused(
    attended, out_weight, residual, norm_gain, expert_ids, route_weights,
    gate_weight, up_weight, down_weight,
):
    rows, width = residual.shape
    sp_count, tp_count = lax.axis_size("sp"), lax.axis_size("tp")
    experts = sp_count * tp_count
    top_k = expert_ids.shape[1]
    capacity = max(2, 2 * top_k * rows // experts)
    hidden = gate_weight.shape[2]
    depth = out_weight.shape[0]
    pieces = 4
    chips = tp_count // 2
    part = (chips, pieces, rows, width // pieces)
    box = (experts, capacity, width)
    vmem = pl.BlockSpec(memory_space=pltpu.VMEM)
    hbm = pl.BlockSpec(memory_space=pl.ANY)
    dma = pltpu.SemaphoreType.DMA
    return pl.pallas_call(
        functools.partial(tail_kernel, (sp_count, tp_count, pieces, capacity)),
        out_shape=jax.ShapeDtypeStruct((rows, width), BF16),
        in_specs=[vmem, hbm, vmem, vmem, vmem, vmem, hbm, hbm, hbm],
        out_specs=vmem,
        scratch_shapes=[
            pltpu.VMEM((depth, width), BF16),
            pltpu.VMEM((width, hidden), BF16),
            pltpu.VMEM((width, hidden), BF16),
            pltpu.VMEM((hidden, width), BF16),
            pltpu.VMEM(part, BF16),
            pltpu.VMEM(part, BF16),
            pltpu.VMEM(part, BF16),
            pltpu.VMEM(part, BF16),
            pltpu.VMEM((rows, width), BF16),
            pltpu.VMEM((rows, width), BF16),
            pltpu.VMEM((rows, experts * capacity), BF16),
            pltpu.VMEM((rows, experts * capacity), BF16),
            pltpu.VMEM((rows, experts * capacity), BF16),
            pltpu.VMEM(box, BF16),
            pltpu.VMEM(box, BF16),
            pltpu.VMEM(box, BF16),
            pltpu.VMEM(box, BF16),
            dma((4,)),
            dma((chips, pieces)),
            dma((chips, pieces)),
            dma((chips, pieces)),
            dma((chips, pieces)),
            dma((experts,)),
            dma((experts,)),
            dma((experts,)),
            dma((experts,)),
        ],
        compiler_params=pltpu.CompilerParams(
            collective_id=0, has_side_effects=True, vmem_limit_bytes=VMEM_BUDGET
        ),
    )(
        attended, out_weight, residual, norm_gain[None], expert_ids, route_weights,
        gate_weight, up_weight, down_weight,
    )


def on_device(queries, key_heads, value_heads, sink_logit, *rest):
    attended = attention(queries, key_heads, value_heads, sink_logit)
    rows_dev = rest[1].shape[0]
    experts = lax.axis_size("sp") * lax.axis_size("tp")
    fits = 2 * rest[3].shape[1] * rows_dev // experts % 16 == 0
    return (tail_fused if fits else tail_plain)(attended, *rest)


def solution(mesh):
    return jax.shard_map(
        on_device,
        mesh=mesh,
        in_specs=(
            P(("grp", "sp"), "tp"),
            P(("grp", "sp"), "tp", None),
            P(("grp", "sp"), "tp", None),
            P("tp"),
            P("tp", None),
            P(("grp", "sp", "tp"), None),
            P(),
            P(("grp", "sp", "tp"), None),
            P(("grp", "sp", "tp"), None),
            P(("sp", "tp"), None, None),
            P(("sp", "tp"), None, None),
            P(("sp", "tp"), None, None),
        ),
        out_specs=P(("grp", "sp", "tp"), None),
        check_vma=False,
    )
```

```python
import functools

import jax
import jax.numpy as jnp
from jax import lax
from jax.experimental import pallas as pl
from jax.experimental.pallas import tpu as pltpu
from jax.sharding import PartitionSpec as P

WINDOW = 128


EPS = 1e-06

F32 = jnp.float32
BF16 = jnp.bfloat16
MESH = pl.DeviceIdType.MESH
VMEM_BUDGET = 56 * 1024 * 1024


def from_behind(value, axis, steps):
    count = lax.axis_size(axis)
    initial, last = (max(0, -steps), min(count, count - steps))
    return lax.ppermute(value, axis, [(source, source + steps) for source in range(initial, last)])


def dot(a, b, dims=((1,), (0,))):
    return lax.dot_general(a, b, (dims, ((), ())), preferred_element_type=F32)


def attention(queries, key_heads, value_heads, sink_logit):
    rows_sp = queries.shape[0]
    kv_local = key_heads.shape[1]
    head_dim = key_heads.shape[2]
    heads_local = queries.shape[1] // head_dim
    group_size = heads_local // kv_local
    window = WINDOW
    count_of_blocks = rows_sp // window
    edge = jnp.stack([key_heads[rows_sp - window :], value_heads[rows_sp - window :]])
    tail_rows = from_behind(edge, "sp", 1)
    key_blocks = jnp.concatenate([tail_rows[0], key_heads], 0).reshape(
        count_of_blocks + 1, window, kv_local, head_dim
    )
    value_blocks = jnp.concatenate([tail_rows[1], value_heads], 0).reshape(
        count_of_blocks + 1, window, kv_local, head_dim
    )
    key_span = jnp.concatenate([key_blocks[:-1], key_blocks[1:]], 1)
    value_span = jnp.concatenate([value_blocks[:-1], value_blocks[1:]], 1)
    query_pos = jnp.arange(window, dtype=jnp.int32)[:, None]
    key_pos = jnp.arange(2 * window, dtype=jnp.int32)[None, :]
    distance = query_pos + window - key_pos
    band = (distance >= 0) & (distance < window)
    key_start = (
        lax.axis_index("sp") * rows_sp
        + jnp.arange(count_of_blocks, dtype=jnp.int32)[:, None] * window
        - window
        + key_pos
    )
    allowed = band[None, :, :] & (key_start >= 0)[:, None, :]
    query_blocks = queries.reshape(count_of_blocks, window, kv_local, group_size, head_dim)
    logit_scores = jnp.einsum(
        "bqhgd,bkhd->bhgqk", query_blocks, key_span, preferred_element_type=jnp.float32
    ) * head_dim ** (-0.5)
    logit_scores = jnp.where(allowed[:, None, None], logit_scores, -jnp.inf)
    sink_col = sink_logit.reshape(kv_local, group_size)[None, :, :, None, None]
    row_max = jnp.maximum(jnp.max(logit_scores, axis=-1, keepdims=True), sink_col)
    expd = jnp.exp(logit_scores - row_max)
    row_total = jnp.sum(expd, axis=-1, keepdims=True) + jnp.exp(sink_col - row_max)
    attention_probabilities = (expd / row_total).astype(jnp.bfloat16)
    attended = jnp.einsum(
        "bhgqk,bkhd->bqhgd", attention_probabilities, value_span, preferred_element_type=jnp.float32
    ).astype(jnp.bfloat16)
    return attended.reshape(rows_sp, heads_local * head_dim)


def tail_plain(
    attended, out_weight, residual, norm_gain, expert_ids, route_weights,
    gate_weight, up_weight, down_weight,
):
    rows_dev = residual.shape[0]
    width = residual.shape[1]
    projected = lax.psum_scatter(
        jnp.dot(attended, out_weight, preferred_element_type=jnp.float32),
        "tp",
        scatter_dimension=0,
        tiled=True,
    )
    stream = (residual.astype(jnp.float32) + projected).astype(jnp.bfloat16)
    wide = stream.astype(jnp.float32)
    normed = (
        wide * lax.rsqrt(jnp.mean(wide * wide, axis=-1, keepdims=True) + EPS) * norm_gain
    ).astype(jnp.bfloat16)
    sp_count = lax.axis_size("sp")
    tp_count = lax.axis_size("tp")
    experts_total = sp_count * tp_count
    top_k = expert_ids.shape[1]
    capacity = max(2, 2 * top_k * rows_dev // experts_total)
    flat_ids = expert_ids.reshape(-1)
    pairs = flat_ids.shape[0]
    onehot = (flat_ids[:, None] == jnp.arange(experts_total, dtype=jnp.int32)[None, :]).astype(
        jnp.int32
    )
    earlier = jnp.cumsum(onehot, axis=0) - onehot
    slot_rank = jnp.sum(earlier * onehot, axis=1)
    flat_slot = flat_ids * capacity + slot_rank
    owner_row = jnp.arange(pairs, dtype=jnp.int32) // top_k
    token_in_slot = jnp.zeros((experts_total * capacity,), jnp.int32).at[flat_slot].set(owner_row)
    filled = jnp.zeros((experts_total * capacity,), jnp.bool_).at[flat_slot].set(True)
    outbox = jnp.where(filled[:, None], normed[token_in_slot], jnp.zeros((), jnp.bfloat16))
    outbox = outbox.reshape(experts_total, capacity, width)
    arrived = lax.all_to_all(outbox, ("sp", "tp"), split_axis=0, concat_axis=0, tiled=True)
    rows = arrived.reshape(-1, width)
    gate = jnp.dot(rows, gate_weight[0], preferred_element_type=jnp.float32)
    upward = jnp.dot(rows, up_weight[0], preferred_element_type=jnp.float32)
    expert_hidden = (jax.nn.silu(gate) * upward).astype(jnp.bfloat16)
    expert_rows = jnp.dot(expert_hidden, down_weight[0], preferred_element_type=jnp.float32).astype(
        jnp.bfloat16
    )
    results = expert_rows.reshape(arrived.shape)
    returned = lax.all_to_all(results, ("sp", "tp"), split_axis=0, concat_axis=0, tiled=True)
    picked_rows = returned.reshape(experts_total * capacity, width)[flat_slot].reshape(
        rows_dev, top_k, width
    )
    shares = route_weights / jnp.sum(route_weights, axis=-1, keepdims=True)
    combined = jnp.sum(shares[:, :, None] * picked_rows.astype(jnp.float32), axis=1)
    return (wide + combined).astype(jnp.bfloat16)


def routing(ids, weights, experts, capacity):
    rows, top_k = ids.shape
    expert = lax.broadcasted_iota(jnp.int32, (rows, experts), 1)
    total = jnp.sum(weights, axis=1, keepdims=True)
    member = jnp.zeros((rows, experts), F32)
    share = jnp.zeros((rows, experts), F32)
    for k in range(top_k):
        hit = (ids[:, k : k + 1] == expert).astype(F32)
        member = member + hit
        share = share + hit * (weights[:, k : k + 1] / total)
    before = (
        lax.broadcasted_iota(jnp.int32, (rows, rows), 0)
        > lax.broadcasted_iota(jnp.int32, (rows, rows), 1)
    ).astype(BF16)
    rank = dot(before, member.astype(BF16))
    rank = jnp.where(member > 0, rank, -1.0)
    slots = experts * capacity
    spread = (
        lax.broadcasted_iota(jnp.int32, (experts, slots), 1) // capacity
        == lax.broadcasted_iota(jnp.int32, (experts, slots), 0)
    ).astype(BF16)
    rank_slot = dot(rank.astype(BF16), spread)
    place = lax.broadcasted_iota(jnp.int32, (rows, slots), 1) % capacity
    taken = rank_slot == place.astype(F32)
    high = share.astype(BF16)
    low = (share - high.astype(F32)).astype(BF16)
    one = jnp.where(taken, 1.0, 0.0)
    return (
        one.astype(BF16),
        (one * dot(high, spread)).astype(BF16),
        (one * dot(low, spread)).astype(BF16),
    )


def attend(sp_count, z, queries, kv, sink, halo, attended, send, recv):
    rows, lanes = kv.shape
    window = halo.shape[0]
    heads = sink.shape[1]
    size = queries.shape[1] // heads
    groups = lanes // (2 * size)
    share = heads // groups
    copy = pltpu.make_async_remote_copy(
        kv.at[pl.ds(rows - window, window)], halo, send, recv,
        device_id={"sp": jnp.minimum(z + 1, sp_count - 1)}, device_id_type=MESH,
    )

    @pl.when(z < sp_count - 1)
    def _():
        copy.start()

    distance = (
        lax.broadcasted_iota(jnp.int32, (window, 2 * window), 0)
        + window
        - lax.broadcasted_iota(jnp.int32, (window, 2 * window), 1)
    )
    band = (distance >= 0) & (distance < window)
    key = lax.broadcasted_iota(jnp.int32, (window, 2 * window), 1)

    def block(b):
        allowed = band
        if b == 0:
            allowed = band & (z * rows - window + key >= 0)
            span = jnp.concatenate([halo[...], kv[:window]], 0)
        else:
            span = kv[(b - 1) * window : (b + 1) * window]
        here = slice(b * window, (b + 1) * window)
        done = []
        for h in range(heads):
            g = h // share
            keys = span[:, 2 * g * size : (2 * g + 1) * size]
            values = span[:, (2 * g + 1) * size : (2 * g + 2) * size]
            score = dot(queries[here, h * size : (h + 1) * size], keys, ((1,), (1,))) * size**-0.5
            score = jnp.where(allowed, score, -1e30)
            drain = sink[0:1, h : h + 1]
            top = jnp.maximum(jnp.max(score, axis=1, keepdims=True), drain)
            grown = jnp.exp(score - top)
            total = jnp.sum(grown, axis=1, keepdims=True) + jnp.exp(drain - top)
            done.append(dot((grown * (1.0 / total)).astype(BF16), values).astype(BF16))
        attended[here, :] = jnp.concatenate(done, 1)

    for b in range(1, rows // window):
        block(b)

    @pl.when(z == 0)
    def _():
        halo[...] = jnp.zeros_like(halo)

    @pl.when(z > 0)
    def _():
        copy.wait_recv()

    block(0)

    @pl.when(z < sp_count - 1)
    def _():
        copy.wait_send()


def tail_kernel(
    sizes,
    queries, kv, sink, out_w_hbm, residual, gain, ids, weights, gate_hbm, up_hbm, down_hbm,
    out,
    halo, attended, halo_send, halo_recv,
    out_w, gate_w, up_w, down_w,
    pair_out, pair_in, far_out, far_in,
    stream, normed, slots, share_hi, share_lo,
    outbox, arrived, results, returned,
    load_sem, pair_send, pair_recv, far_send, far_recv,
    go_send, go_recv, back_send, back_recv,
):
    sp_count, tp_count, pieces, capacity = sizes
    experts = sp_count * tp_count
    chips = tp_count // 2
    z, t = lax.axis_index("sp"), lax.axis_index("tp")
    me = z * tp_count + t
    x, core = t // 2, t % 2
    other = 1 - core
    rows, width = residual.shape
    piece = width // pieces

    def where(e):
        return {"sp": e // tp_count, "tp": e % tp_count}

    loads = [
        pltpu.make_async_copy(src, dst, load_sem.at[i])
        for i, (src, dst) in enumerate(
            ((out_w_hbm, out_w), (gate_hbm.at[0], gate_w), (up_hbm.at[0], up_w), (down_hbm.at[0], down_w))
        )
    ]
    for load in loads:
        load.start()

    barrier = pltpu.get_barrier_semaphore()

    def greet(k, carry):
        pl.semaphore_signal(
            barrier, inc=1, device_id=where((me + k) % experts), device_id_type=MESH
        )
        return carry

    lax.fori_loop(1, experts, greet, 0)
    pl.semaphore_wait(barrier, experts - 1)
    attend(sp_count, z, queries, kv, sink, halo, attended, halo_send, halo_recv)
    loads[0].wait()

    def partial(chip, which, q):
        block = attended[pl.ds(pl.multiple_of((chip * 2 + which) * rows, rows), rows), :]
        return dot(block, out_w[:, q * piece : (q + 1) * piece])

    def pair_copy(k, q):
        return pltpu.make_async_remote_copy(
            pair_out.at[k, q], pair_in.at[k, q], pair_send.at[k, q], pair_recv.at[k, q],
            device_id={"tp": x * 2 + other}, device_id_type=MESH,
        )

    def far_copy(k, q):
        return pltpu.make_async_remote_copy(
            far_out.at[k, q], far_in.at[k, q], far_send.at[k, q], far_recv.at[k, q],
            device_id={"tp": ((x + k) % chips) * 2 + core}, device_id_type=MESH,
        )

    order = list(range(1, chips)) + [0]
    for q in range(pieces):
        for k in order:
            pair_out[k, q] = partial((x + k) % chips, other, q).astype(BF16)
            pair_copy(k, q).start()
        for k in range(1, chips):
            mine = partial((x + k) % chips, core, q)
            pair_copy(k, q).wait_recv()
            far_out[k, q] = (mine + pair_in[k, q].astype(F32)).astype(BF16)
            far_copy(k, q).start()
    slots[...], share_hi[...], share_lo[...] = routing(ids[...], weights[...], experts, capacity)
    square = jnp.zeros((rows, 1), F32)
    for q in range(pieces):
        cols = slice(q * piece, (q + 1) * piece)
        total = partial(x, core, q)
        pair_copy(0, q).wait_recv()
        total = total + pair_in[0, q].astype(F32)
        for k in range(1, chips):
            far_copy(k, q).wait_recv()
            total = total + far_in[k, q].astype(F32)
        value = (residual[:, cols].astype(F32) + total).astype(BF16)
        stream[:, cols] = value
        value = value.astype(F32)
        square = square + jnp.sum(value * value, axis=1, keepdims=True)
    scale = lax.rsqrt(square / width + EPS)
    for q in range(pieces):
        cols = slice(q * piece, (q + 1) * piece)
        normed[:, cols] = (stream[:, cols].astype(F32) * scale * gain[:, cols]).astype(BF16)

    def go_copy(to, at):
        return pltpu.make_async_remote_copy(
            outbox.at[to], arrived.at[at], go_send.at[to], go_recv.at[at],
            device_id=where(to), device_id_type=MESH,
        )

    def back_copy(to, at):
        return pltpu.make_async_remote_copy(
            results.at[to], returned.at[at], back_send.at[to], back_recv.at[at],
            device_id=where(to), device_id_type=MESH,
        )

    picks = tp_count * capacity
    for d in range(sp_count):
        layer = range(d * tp_count, (d + 1) * tp_count)
        chosen = dot(slots[:, d * picks : (d + 1) * picks], normed[...], ((0,), (0,))).astype(BF16)
        for i, e in enumerate(layer):
            outbox[e] = chosen[i * capacity : (i + 1) * capacity]

            @pl.when(e != me)
            def _():
                go_copy(e, me).start()

    arrived[me] = outbox[me]
    for load in loads[1:]:
        load.wait()

    def expert(d, carry):
        layer = (z + d) % sp_count
        for i in range(tp_count):
            e = layer * tp_count + i

            @pl.when(e != me)
            def _():
                go_copy(me, e).wait_recv()

        block = arrived[pl.ds(layer * tp_count, tp_count)].reshape(picks, width)
        gated = dot(block, gate_w[...])
        raised = dot(block, up_w[...])
        hidden = (gated / (1.0 + jnp.exp(-gated)) * raised).astype(BF16)
        done = dot(hidden, down_w[...]).astype(BF16)
        results[pl.ds(layer * tp_count, tp_count)] = done.reshape(tp_count, capacity, width)
        for i in range(tp_count):
            e = layer * tp_count + i

            @pl.when(e != me)
            def _():
                back_copy(e, me).start()

        return carry

    lax.fori_loop(0, sp_count, expert, 0)
    returned[me] = results[me]

    def collect(k, carry):
        e = (me + k) % experts
        back_copy(me, e).wait_recv()
        return carry

    lax.fori_loop(1, experts, collect, 0)
    for q in range(pieces):
        cols = slice(q * piece, (q + 1) * piece)
        back = returned[:, :, cols].reshape(experts * capacity, piece)
        mixed = dot(share_hi[...], back) + dot(share_lo[...], back)
        out[:, cols] = (stream[:, cols].astype(F32) + mixed).astype(BF16)

    for q in range(pieces):
        for k in range(chips):
            pair_copy(k, q).wait_send()
            if k:
                far_copy(k, q).wait_send()

    def flush(k, carry):
        e = (me + k) % experts
        go_copy(e, me).wait_send()
        back_copy(e, me).wait_send()
        return carry

    lax.fori_loop(1, experts, flush, 0)


def fused(
    queries, key_heads, value_heads, sink_logit, out_weight, residual, norm_gain, expert_ids, route_weights,
    gate_weight, up_weight, down_weight,
):
    rows, width = residual.shape
    sp_count, tp_count = lax.axis_size("sp"), lax.axis_size("tp")
    experts = sp_count * tp_count
    top_k = expert_ids.shape[1]
    capacity = max(2, 2 * top_k * rows // experts)
    hidden = gate_weight.shape[2]
    depth = out_weight.shape[0]
    pieces = 4
    chips = tp_count // 2
    part = (chips, pieces, rows, width // pieces)
    box = (experts, capacity, width)
    seen, groups, size = key_heads.shape
    kv = jnp.stack([key_heads, value_heads], 2).reshape(seen, groups * 2 * size)
    vmem = pl.BlockSpec(memory_space=pltpu.VMEM)
    hbm = pl.BlockSpec(memory_space=pl.ANY)
    dma = pltpu.SemaphoreType.DMA
    return pl.pallas_call(
        functools.partial(tail_kernel, (sp_count, tp_count, pieces, capacity)),
        out_shape=jax.ShapeDtypeStruct((rows, width), BF16),
        in_specs=[vmem, vmem, vmem, hbm, vmem, vmem, vmem, vmem, hbm, hbm, hbm],
        out_specs=vmem,
        scratch_shapes=[
            pltpu.VMEM((WINDOW, kv.shape[1]), BF16),
            pltpu.VMEM(queries.shape, BF16),
            dma,
            dma,
            pltpu.VMEM((depth, width), BF16),
            pltpu.VMEM((width, hidden), BF16),
            pltpu.VMEM((width, hidden), BF16),
            pltpu.VMEM((hidden, width), BF16),
            pltpu.VMEM(part, BF16),
            pltpu.VMEM(part, BF16),
            pltpu.VMEM(part, BF16),
            pltpu.VMEM(part, BF16),
            pltpu.VMEM((rows, width), BF16),
            pltpu.VMEM((rows, width), BF16),
            pltpu.VMEM((rows, experts * capacity), BF16),
            pltpu.VMEM((rows, experts * capacity), BF16),
            pltpu.VMEM((rows, experts * capacity), BF16),
            pltpu.VMEM(box, BF16),
            pltpu.VMEM(box, BF16),
            pltpu.VMEM(box, BF16),
            pltpu.VMEM(box, BF16),
            dma((4,)),
            dma((chips, pieces)),
            dma((chips, pieces)),
            dma((chips, pieces)),
            dma((chips, pieces)),
            dma((experts,)),
            dma((experts,)),
            dma((experts,)),
            dma((experts,)),
        ],
        compiler_params=pltpu.CompilerParams(
            collective_id=0, has_side_effects=True, vmem_limit_bytes=VMEM_BUDGET
        ),
    )(
        queries, kv, sink_logit[None], out_weight, residual, norm_gain[None], expert_ids, route_weights,
        gate_weight, up_weight, down_weight,
    )


def on_device(queries, key_heads, value_heads, sink_logit, *rest):
    rows_dev = rest[1].shape[0]
    experts = lax.axis_size("sp") * lax.axis_size("tp")
    fits = 2 * rest[3].shape[1] * rows_dev // experts % 16 == 0
    if fits:
        return fused(queries, key_heads, value_heads, sink_logit, *rest)
    return tail_plain(attention(queries, key_heads, value_heads, sink_logit), *rest)


def solution(mesh):
    return jax.shard_map(
        on_device,
        mesh=mesh,
        in_specs=(
            P(("grp", "sp"), "tp"),
            P(("grp", "sp"), "tp", None),
            P(("grp", "sp"), "tp", None),
            P("tp"),
            P("tp", None),
            P(("grp", "sp", "tp"), None),
            P(),
            P(("grp", "sp", "tp"), None),
            P(("grp", "sp", "tp"), None),
            P(("sp", "tp"), None, None),
            P(("sp", "tp"), None, None),
            P(("sp", "tp"), None, None),
        ),
        out_specs=P(("grp", "sp", "tp"), None),
        check_vma=False,
    )
```

```python
import functools

import jax
import jax.numpy as jnp
from jax import lax
from jax.experimental import pallas as pl
from jax.experimental.pallas import tpu as pltpu
from jax.sharding import PartitionSpec as P

WINDOW = 128


EPS = 1e-06

F32 = jnp.float32
BF16 = jnp.bfloat16
MESH = pl.DeviceIdType.MESH
VMEM_BUDGET = 56 * 1024 * 1024


def from_behind(value, axis, steps):
    count = lax.axis_size(axis)
    initial, last = (max(0, -steps), min(count, count - steps))
    return lax.ppermute(value, axis, [(source, source + steps) for source in range(initial, last)])


def dot(a, b, dims=((1,), (0,))):
    return lax.dot_general(a, b, (dims, ((), ())), preferred_element_type=F32)


def attention(queries, key_heads, value_heads, sink_logit):
    rows_sp = queries.shape[0]
    kv_local = key_heads.shape[1]
    head_dim = key_heads.shape[2]
    heads_local = queries.shape[1] // head_dim
    group_size = heads_local // kv_local
    window = WINDOW
    count_of_blocks = rows_sp // window
    edge = jnp.stack([key_heads[rows_sp - window :], value_heads[rows_sp - window :]])
    tail_rows = from_behind(edge, "sp", 1)
    key_blocks = jnp.concatenate([tail_rows[0], key_heads], 0).reshape(
        count_of_blocks + 1, window, kv_local, head_dim
    )
    value_blocks = jnp.concatenate([tail_rows[1], value_heads], 0).reshape(
        count_of_blocks + 1, window, kv_local, head_dim
    )
    key_span = jnp.concatenate([key_blocks[:-1], key_blocks[1:]], 1)
    value_span = jnp.concatenate([value_blocks[:-1], value_blocks[1:]], 1)
    query_pos = jnp.arange(window, dtype=jnp.int32)[:, None]
    key_pos = jnp.arange(2 * window, dtype=jnp.int32)[None, :]
    distance = query_pos + window - key_pos
    band = (distance >= 0) & (distance < window)
    key_start = (
        lax.axis_index("sp") * rows_sp
        + jnp.arange(count_of_blocks, dtype=jnp.int32)[:, None] * window
        - window
        + key_pos
    )
    allowed = band[None, :, :] & (key_start >= 0)[:, None, :]
    query_blocks = queries.reshape(count_of_blocks, window, kv_local, group_size, head_dim)
    logit_scores = jnp.einsum(
        "bqhgd,bkhd->bhgqk", query_blocks, key_span, preferred_element_type=jnp.float32
    ) * head_dim ** (-0.5)
    logit_scores = jnp.where(allowed[:, None, None], logit_scores, -jnp.inf)
    sink_col = sink_logit.reshape(kv_local, group_size)[None, :, :, None, None]
    row_max = jnp.maximum(jnp.max(logit_scores, axis=-1, keepdims=True), sink_col)
    expd = jnp.exp(logit_scores - row_max)
    row_total = jnp.sum(expd, axis=-1, keepdims=True) + jnp.exp(sink_col - row_max)
    attention_probabilities = (expd / row_total).astype(jnp.bfloat16)
    attended = jnp.einsum(
        "bhgqk,bkhd->bqhgd", attention_probabilities, value_span, preferred_element_type=jnp.float32
    ).astype(jnp.bfloat16)
    return attended.reshape(rows_sp, heads_local * head_dim)


def tail_plain(
    attended, out_weight, residual, norm_gain, expert_ids, route_weights,
    gate_weight, up_weight, down_weight,
):
    rows_dev = residual.shape[0]
    width = residual.shape[1]
    projected = lax.psum_scatter(
        jnp.dot(attended, out_weight, preferred_element_type=jnp.float32),
        "tp",
        scatter_dimension=0,
        tiled=True,
    )
    stream = (residual.astype(jnp.float32) + projected).astype(jnp.bfloat16)
    wide = stream.astype(jnp.float32)
    normed = (
        wide * lax.rsqrt(jnp.mean(wide * wide, axis=-1, keepdims=True) + EPS) * norm_gain
    ).astype(jnp.bfloat16)
    sp_count = lax.axis_size("sp")
    tp_count = lax.axis_size("tp")
    experts_total = sp_count * tp_count
    top_k = expert_ids.shape[1]
    capacity = max(2, 2 * top_k * rows_dev // experts_total)
    flat_ids = expert_ids.reshape(-1)
    pairs = flat_ids.shape[0]
    onehot = (flat_ids[:, None] == jnp.arange(experts_total, dtype=jnp.int32)[None, :]).astype(
        jnp.int32
    )
    earlier = jnp.cumsum(onehot, axis=0) - onehot
    slot_rank = jnp.sum(earlier * onehot, axis=1)
    flat_slot = flat_ids * capacity + slot_rank
    owner_row = jnp.arange(pairs, dtype=jnp.int32) // top_k
    token_in_slot = jnp.zeros((experts_total * capacity,), jnp.int32).at[flat_slot].set(owner_row)
    filled = jnp.zeros((experts_total * capacity,), jnp.bool_).at[flat_slot].set(True)
    outbox = jnp.where(filled[:, None], normed[token_in_slot], jnp.zeros((), jnp.bfloat16))
    outbox = outbox.reshape(experts_total, capacity, width)
    arrived = lax.all_to_all(outbox, ("sp", "tp"), split_axis=0, concat_axis=0, tiled=True)
    rows = arrived.reshape(-1, width)
    gate = jnp.dot(rows, gate_weight[0], preferred_element_type=jnp.float32)
    upward = jnp.dot(rows, up_weight[0], preferred_element_type=jnp.float32)
    expert_hidden = (jax.nn.silu(gate) * upward).astype(jnp.bfloat16)
    expert_rows = jnp.dot(expert_hidden, down_weight[0], preferred_element_type=jnp.float32).astype(
        jnp.bfloat16
    )
    results = expert_rows.reshape(arrived.shape)
    returned = lax.all_to_all(results, ("sp", "tp"), split_axis=0, concat_axis=0, tiled=True)
    picked_rows = returned.reshape(experts_total * capacity, width)[flat_slot].reshape(
        rows_dev, top_k, width
    )
    shares = route_weights / jnp.sum(route_weights, axis=-1, keepdims=True)
    combined = jnp.sum(shares[:, :, None] * picked_rows.astype(jnp.float32), axis=1)
    return (wide + combined).astype(jnp.bfloat16)


def routing(ids, weights, experts, capacity):
    rows, top_k = ids.shape
    expert = lax.broadcasted_iota(jnp.int32, (rows, experts), 1)
    total = jnp.sum(weights, axis=1, keepdims=True)
    member = jnp.zeros((rows, experts), F32)
    share = jnp.zeros((rows, experts), F32)
    for k in range(top_k):
        hit = (ids[:, k : k + 1] == expert).astype(F32)
        member = member + hit
        share = share + hit * (weights[:, k : k + 1] / total)
    before = (
        lax.broadcasted_iota(jnp.int32, (rows, rows), 0)
        > lax.broadcasted_iota(jnp.int32, (rows, rows), 1)
    ).astype(BF16)
    rank = dot(before, member.astype(BF16))
    rank = jnp.where(member > 0, rank, -1.0)
    slots = experts * capacity
    spread = (
        lax.broadcasted_iota(jnp.int32, (experts, slots), 1) // capacity
        == lax.broadcasted_iota(jnp.int32, (experts, slots), 0)
    ).astype(BF16)
    rank_slot = dot(rank.astype(BF16), spread)
    place = lax.broadcasted_iota(jnp.int32, (rows, slots), 1) % capacity
    taken = rank_slot == place.astype(F32)
    high = share.astype(BF16)
    low = (share - high.astype(F32)).astype(BF16)
    one = jnp.where(taken, 1.0, 0.0)
    return (
        one.astype(BF16),
        (one * dot(high, spread)).astype(BF16),
        (one * dot(low, spread)).astype(BF16),
    )


def attend(sp_count, z, queries, kv, sink, halo, attended, send, recv):
    rows, lanes = kv.shape
    window = halo.shape[0]
    heads = sink.shape[1]
    size = queries.shape[1] // heads
    groups = lanes // (2 * size)
    share = heads // groups
    copy = pltpu.make_async_remote_copy(
        kv.at[pl.ds(rows - window, window)], halo, send, recv,
        device_id={"sp": jnp.minimum(z + 1, sp_count - 1)}, device_id_type=MESH,
    )

    @pl.when(z < sp_count - 1)
    def _():
        copy.start()

    pairs = share // 2
    tall = pairs * window
    query = lax.broadcasted_iota(jnp.int32, (tall, 2 * window), 0) % window
    key = lax.broadcasted_iota(jnp.int32, (tall, 2 * window), 1)
    distance = query + window - key
    band = (distance >= 0) & (distance < window)

    def block(b):
        allowed = band
        if b == 0:
            allowed = band & (z * rows - window + key >= 0)
            span = jnp.concatenate([halo[...], kv[:window]], 0)
        else:
            span = kv[(b - 1) * window : (b + 1) * window]
        here = slice(b * window, (b + 1) * window)
        for g in range(groups):
            keys = span[:, 2 * g * size : (2 * g + 1) * size]
            values = span[:, (2 * g + 1) * size : (2 * g + 2) * size]
            none, ones = jnp.zeros_like(keys), jnp.ones_like(values)
            wide = jnp.concatenate(
                [
                    queries[here, (g * share + 2 * i) * size : (g * share + 2 * i + 2) * size]
                    for i in range(pairs)
                ],
                0,
            )
            sides = []
            for odd in range(2):
                two_keys = jnp.concatenate([none, keys] if odd else [keys, none], 1)
                two_values = jnp.concatenate([ones, values] if odd else [values, ones], 1)
                score = dot(wide, two_keys, ((1,), (1,))) * size**-0.5
                score = jnp.where(allowed, score, -1e30)
                drain = jnp.concatenate(
                    [
                        jnp.broadcast_to(
                            sink[0:1, g * share + 2 * i + odd : g * share + 2 * i + odd + 1],
                            (window, 1),
                        )
                        for i in range(pairs)
                    ],
                    0,
                )
                top = jnp.maximum(jnp.max(score, axis=1, keepdims=True), drain)
                grown = jnp.exp(score - top).astype(BF16)
                both = dot(grown, two_values)
                at = 0 if odd else size
                total = both[:, at : at + 1] + jnp.exp(drain - top)
                sides.append(both * (1.0 / total))
            lane = lax.broadcasted_iota(jnp.int32, (tall, 2 * size), 1)
            both = jnp.where(lane < size, sides[0], sides[1]).astype(BF16)
            for i in range(pairs):
                first = (g * share + 2 * i) * size
                attended[here, first : first + 2 * size] = both[i * window : (i + 1) * window]

    for b in range(1, rows // window):
        block(b)

    @pl.when(z == 0)
    def _():
        halo[...] = jnp.zeros_like(halo)

    @pl.when(z > 0)
    def _():
        copy.wait_recv()

    block(0)

    @pl.when(z < sp_count - 1)
    def _():
        copy.wait_send()


def tail_kernel(
    sizes,
    queries, kv, sink, out_w_hbm, residual, gain, ids, weights, gate_hbm, up_hbm, down_hbm,
    out,
    halo, attended, halo_send, halo_recv,
    out_w, gate_w, up_w, down_w,
    pair_out, pair_in, far_out, far_in,
    stream, normed, slots, share_hi, share_lo,
    outbox, arrived, results, returned,
    load_sem, pair_send, pair_recv, far_send, far_recv,
    go_send, go_recv, back_send, back_recv,
):
    sp_count, tp_count, pieces, capacity = sizes
    experts = sp_count * tp_count
    chips = tp_count // 2
    z, t = lax.axis_index("sp"), lax.axis_index("tp")
    me = z * tp_count + t
    x, core = t // 2, t % 2
    other = 1 - core
    rows, width = residual.shape
    piece = width // pieces

    def where(e):
        return {"sp": e // tp_count, "tp": e % tp_count}

    loads = [
        pltpu.make_async_copy(src, dst, load_sem.at[i])
        for i, (src, dst) in enumerate(
            ((out_w_hbm, out_w), (gate_hbm.at[0], gate_w), (up_hbm.at[0], up_w), (down_hbm.at[0], down_w))
        )
    ]
    for load in loads:
        load.start()

    barrier = pltpu.get_barrier_semaphore()

    def greet(k, carry):
        pl.semaphore_signal(
            barrier, inc=1, device_id=where((me + k) % experts), device_id_type=MESH
        )
        return carry

    lax.fori_loop(1, experts, greet, 0)
    pl.semaphore_wait(barrier, experts - 1)
    attend(sp_count, z, queries, kv, sink, halo, attended, halo_send, halo_recv)
    loads[0].wait()

    def partial(chip, which, q):
        block = attended[pl.ds(pl.multiple_of((chip * 2 + which) * rows, rows), rows), :]
        return dot(block, out_w[:, q * piece : (q + 1) * piece])

    def pair_copy(k, q):
        return pltpu.make_async_remote_copy(
            pair_out.at[k, q], pair_in.at[k, q], pair_send.at[k, q], pair_recv.at[k, q],
            device_id={"tp": x * 2 + other}, device_id_type=MESH,
        )

    def far_copy(k, q):
        return pltpu.make_async_remote_copy(
            far_out.at[k, q], far_in.at[k, q], far_send.at[k, q], far_recv.at[k, q],
            device_id={"tp": ((x + k) % chips) * 2 + core}, device_id_type=MESH,
        )

    order = list(range(1, chips)) + [0]
    for q in range(pieces):
        for k in order:
            pair_out[k, q] = partial((x + k) % chips, other, q).astype(BF16)
            pair_copy(k, q).start()
        for k in range(1, chips):
            mine = partial((x + k) % chips, core, q)
            pair_copy(k, q).wait_recv()
            far_out[k, q] = (mine + pair_in[k, q].astype(F32)).astype(BF16)
            far_copy(k, q).start()
    slots[...], share_hi[...], share_lo[...] = routing(ids[...], weights[...], experts, capacity)
    square = jnp.zeros((rows, 1), F32)
    for q in range(pieces):
        cols = slice(q * piece, (q + 1) * piece)
        total = partial(x, core, q)
        pair_copy(0, q).wait_recv()
        total = total + pair_in[0, q].astype(F32)
        for k in range(1, chips):
            far_copy(k, q).wait_recv()
            total = total + far_in[k, q].astype(F32)
        value = (residual[:, cols].astype(F32) + total).astype(BF16)
        stream[:, cols] = value
        value = value.astype(F32)
        square = square + jnp.sum(value * value, axis=1, keepdims=True)
    scale = lax.rsqrt(square / width + EPS)
    for q in range(pieces):
        cols = slice(q * piece, (q + 1) * piece)
        normed[:, cols] = (stream[:, cols].astype(F32) * scale * gain[:, cols]).astype(BF16)

    def go_copy(to, at):
        return pltpu.make_async_remote_copy(
            outbox.at[to], arrived.at[at], go_send.at[to], go_recv.at[at],
            device_id=where(to), device_id_type=MESH,
        )

    def back_copy(to, at):
        return pltpu.make_async_remote_copy(
            results.at[to], returned.at[at], back_send.at[to], back_recv.at[at],
            device_id=where(to), device_id_type=MESH,
        )

    picks = tp_count * capacity
    for d in range(sp_count):
        layer = range(d * tp_count, (d + 1) * tp_count)
        chosen = dot(slots[:, d * picks : (d + 1) * picks], normed[...], ((0,), (0,))).astype(BF16)
        for i, e in enumerate(layer):
            outbox[e] = chosen[i * capacity : (i + 1) * capacity]

            @pl.when(e != me)
            def _():
                go_copy(e, me).start()

    arrived[me] = outbox[me]
    for load in loads[1:]:
        load.wait()

    def expert(d, carry):
        layer = (z + d) % sp_count
        for i in range(tp_count):
            e = layer * tp_count + i

            @pl.when(e != me)
            def _():
                go_copy(me, e).wait_recv()

        block = arrived[pl.ds(layer * tp_count, tp_count)].reshape(picks, width)
        gated = dot(block, gate_w[...])
        raised = dot(block, up_w[...])
        hidden = (gated / (1.0 + jnp.exp(-gated)) * raised).astype(BF16)
        done = dot(hidden, down_w[...]).astype(BF16)
        results[pl.ds(layer * tp_count, tp_count)] = done.reshape(tp_count, capacity, width)
        for i in range(tp_count):
            e = layer * tp_count + i

            @pl.when(e != me)
            def _():
                back_copy(e, me).start()

        return carry

    lax.fori_loop(0, sp_count, expert, 0)
    returned[me] = results[me]

    def collect(k, carry):
        e = (me + k) % experts
        back_copy(me, e).wait_recv()
        return carry

    lax.fori_loop(1, experts, collect, 0)
    for q in range(pieces):
        cols = slice(q * piece, (q + 1) * piece)
        back = returned[:, :, cols].reshape(experts * capacity, piece)
        mixed = dot(share_hi[...], back) + dot(share_lo[...], back)
        out[:, cols] = (stream[:, cols].astype(F32) + mixed).astype(BF16)

    for q in range(pieces):
        for k in range(chips):
            pair_copy(k, q).wait_send()
            if k:
                far_copy(k, q).wait_send()

    def flush(k, carry):
        e = (me + k) % experts
        go_copy(e, me).wait_send()
        back_copy(e, me).wait_send()
        return carry

    lax.fori_loop(1, experts, flush, 0)


def fused(
    queries, key_heads, value_heads, sink_logit, out_weight, residual, norm_gain, expert_ids, route_weights,
    gate_weight, up_weight, down_weight,
):
    rows, width = residual.shape
    sp_count, tp_count = lax.axis_size("sp"), lax.axis_size("tp")
    experts = sp_count * tp_count
    top_k = expert_ids.shape[1]
    capacity = max(2, 2 * top_k * rows // experts)
    hidden = gate_weight.shape[2]
    depth = out_weight.shape[0]
    pieces = 4
    chips = tp_count // 2
    part = (chips, pieces, rows, width // pieces)
    box = (experts, capacity, width)
    seen, groups, size = key_heads.shape
    kv = jnp.stack([key_heads, value_heads], 2).reshape(seen, groups * 2 * size)
    vmem = pl.BlockSpec(memory_space=pltpu.VMEM)
    hbm = pl.BlockSpec(memory_space=pl.ANY)
    dma = pltpu.SemaphoreType.DMA
    return pl.pallas_call(
        functools.partial(tail_kernel, (sp_count, tp_count, pieces, capacity)),
        out_shape=jax.ShapeDtypeStruct((rows, width), BF16),
        in_specs=[vmem, vmem, vmem, hbm, vmem, vmem, vmem, vmem, hbm, hbm, hbm],
        out_specs=vmem,
        scratch_shapes=[
            pltpu.VMEM((WINDOW, kv.shape[1]), BF16),
            pltpu.VMEM(queries.shape, BF16),
            dma,
            dma,
            pltpu.VMEM((depth, width), BF16),
            pltpu.VMEM((width, hidden), BF16),
            pltpu.VMEM((width, hidden), BF16),
            pltpu.VMEM((hidden, width), BF16),
            pltpu.VMEM(part, BF16),
            pltpu.VMEM(part, BF16),
            pltpu.VMEM(part, BF16),
            pltpu.VMEM(part, BF16),
            pltpu.VMEM((rows, width), BF16),
            pltpu.VMEM((rows, width), BF16),
            pltpu.VMEM((rows, experts * capacity), BF16),
            pltpu.VMEM((rows, experts * capacity), BF16),
            pltpu.VMEM((rows, experts * capacity), BF16),
            pltpu.VMEM(box, BF16),
            pltpu.VMEM(box, BF16),
            pltpu.VMEM(box, BF16),
            pltpu.VMEM(box, BF16),
            dma((4,)),
            dma((chips, pieces)),
            dma((chips, pieces)),
            dma((chips, pieces)),
            dma((chips, pieces)),
            dma((experts,)),
            dma((experts,)),
            dma((experts,)),
            dma((experts,)),
        ],
        compiler_params=pltpu.CompilerParams(
            collective_id=0, has_side_effects=True, vmem_limit_bytes=VMEM_BUDGET
        ),
    )(
        queries, kv, sink_logit[None], out_weight, residual, norm_gain[None], expert_ids, route_weights,
        gate_weight, up_weight, down_weight,
    )


def on_device(queries, key_heads, value_heads, sink_logit, *rest):
    rows_dev = rest[1].shape[0]
    experts = lax.axis_size("sp") * lax.axis_size("tp")
    fits = 2 * rest[3].shape[1] * rows_dev // experts % 16 == 0
    if fits:
        return fused(queries, key_heads, value_heads, sink_logit, *rest)
    return tail_plain(attention(queries, key_heads, value_heads, sink_logit), *rest)


def solution(mesh):
    return jax.shard_map(
        on_device,
        mesh=mesh,
        in_specs=(
            P(("grp", "sp"), "tp"),
            P(("grp", "sp"), "tp", None),
            P(("grp", "sp"), "tp", None),
            P("tp"),
            P("tp", None),
            P(("grp", "sp", "tp"), None),
            P(),
            P(("grp", "sp", "tp"), None),
            P(("grp", "sp", "tp"), None),
            P(("sp", "tp"), None, None),
            P(("sp", "tp"), None, None),
            P(("sp", "tp"), None, None),
        ),
        out_specs=P(("grp", "sp", "tp"), None),
        check_vma=False,
    )
```

```python
import functools

import jax
import jax.numpy as jnp
from jax import lax
from jax.experimental import pallas as pl
from jax.experimental.pallas import tpu as pltpu
from jax.sharding import PartitionSpec as P

WINDOW = 128


EPS = 1e-06

F32 = jnp.float32
BF16 = jnp.bfloat16
MESH = pl.DeviceIdType.MESH
VMEM_BUDGET = 56 * 1024 * 1024


def from_behind(value, axis, steps):
    count = lax.axis_size(axis)
    initial, last = (max(0, -steps), min(count, count - steps))
    return lax.ppermute(value, axis, [(source, source + steps) for source in range(initial, last)])


def dot(a, b, dims=((1,), (0,))):
    return lax.dot_general(a, b, (dims, ((), ())), preferred_element_type=F32)


def attention(queries, key_heads, value_heads, sink_logit):
    rows_sp = queries.shape[0]
    kv_local = key_heads.shape[1]
    head_dim = key_heads.shape[2]
    heads_local = queries.shape[1] // head_dim
    group_size = heads_local // kv_local
    window = WINDOW
    count_of_blocks = rows_sp // window
    edge = jnp.stack([key_heads[rows_sp - window :], value_heads[rows_sp - window :]])
    tail_rows = from_behind(edge, "sp", 1)
    key_blocks = jnp.concatenate([tail_rows[0], key_heads], 0).reshape(
        count_of_blocks + 1, window, kv_local, head_dim
    )
    value_blocks = jnp.concatenate([tail_rows[1], value_heads], 0).reshape(
        count_of_blocks + 1, window, kv_local, head_dim
    )
    key_span = jnp.concatenate([key_blocks[:-1], key_blocks[1:]], 1)
    value_span = jnp.concatenate([value_blocks[:-1], value_blocks[1:]], 1)
    query_pos = jnp.arange(window, dtype=jnp.int32)[:, None]
    key_pos = jnp.arange(2 * window, dtype=jnp.int32)[None, :]
    distance = query_pos + window - key_pos
    band = (distance >= 0) & (distance < window)
    key_start = (
        lax.axis_index("sp") * rows_sp
        + jnp.arange(count_of_blocks, dtype=jnp.int32)[:, None] * window
        - window
        + key_pos
    )
    allowed = band[None, :, :] & (key_start >= 0)[:, None, :]
    query_blocks = queries.reshape(count_of_blocks, window, kv_local, group_size, head_dim)
    logit_scores = jnp.einsum(
        "bqhgd,bkhd->bhgqk", query_blocks, key_span, preferred_element_type=jnp.float32
    ) * head_dim ** (-0.5)
    logit_scores = jnp.where(allowed[:, None, None], logit_scores, -jnp.inf)
    sink_col = sink_logit.reshape(kv_local, group_size)[None, :, :, None, None]
    row_max = jnp.maximum(jnp.max(logit_scores, axis=-1, keepdims=True), sink_col)
    expd = jnp.exp(logit_scores - row_max)
    row_total = jnp.sum(expd, axis=-1, keepdims=True) + jnp.exp(sink_col - row_max)
    attention_probabilities = (expd / row_total).astype(jnp.bfloat16)
    attended = jnp.einsum(
        "bhgqk,bkhd->bqhgd", attention_probabilities, value_span, preferred_element_type=jnp.float32
    ).astype(jnp.bfloat16)
    return attended.reshape(rows_sp, heads_local * head_dim)


def tail_plain(
    attended, out_weight, residual, norm_gain, expert_ids, route_weights,
    gate_weight, up_weight, down_weight,
):
    rows_dev = residual.shape[0]
    width = residual.shape[1]
    projected = lax.psum_scatter(
        jnp.dot(attended, out_weight, preferred_element_type=jnp.float32),
        "tp",
        scatter_dimension=0,
        tiled=True,
    )
    stream = (residual.astype(jnp.float32) + projected).astype(jnp.bfloat16)
    wide = stream.astype(jnp.float32)
    normed = (
        wide * lax.rsqrt(jnp.mean(wide * wide, axis=-1, keepdims=True) + EPS) * norm_gain
    ).astype(jnp.bfloat16)
    sp_count = lax.axis_size("sp")
    tp_count = lax.axis_size("tp")
    experts_total = sp_count * tp_count
    top_k = expert_ids.shape[1]
    capacity = max(2, 2 * top_k * rows_dev // experts_total)
    flat_ids = expert_ids.reshape(-1)
    pairs = flat_ids.shape[0]
    onehot = (flat_ids[:, None] == jnp.arange(experts_total, dtype=jnp.int32)[None, :]).astype(
        jnp.int32
    )
    earlier = jnp.cumsum(onehot, axis=0) - onehot
    slot_rank = jnp.sum(earlier * onehot, axis=1)
    flat_slot = flat_ids * capacity + slot_rank
    owner_row = jnp.arange(pairs, dtype=jnp.int32) // top_k
    token_in_slot = jnp.zeros((experts_total * capacity,), jnp.int32).at[flat_slot].set(owner_row)
    filled = jnp.zeros((experts_total * capacity,), jnp.bool_).at[flat_slot].set(True)
    outbox = jnp.where(filled[:, None], normed[token_in_slot], jnp.zeros((), jnp.bfloat16))
    outbox = outbox.reshape(experts_total, capacity, width)
    arrived = lax.all_to_all(outbox, ("sp", "tp"), split_axis=0, concat_axis=0, tiled=True)
    rows = arrived.reshape(-1, width)
    gate = jnp.dot(rows, gate_weight[0], preferred_element_type=jnp.float32)
    upward = jnp.dot(rows, up_weight[0], preferred_element_type=jnp.float32)
    expert_hidden = (jax.nn.silu(gate) * upward).astype(jnp.bfloat16)
    expert_rows = jnp.dot(expert_hidden, down_weight[0], preferred_element_type=jnp.float32).astype(
        jnp.bfloat16
    )
    results = expert_rows.reshape(arrived.shape)
    returned = lax.all_to_all(results, ("sp", "tp"), split_axis=0, concat_axis=0, tiled=True)
    picked_rows = returned.reshape(experts_total * capacity, width)[flat_slot].reshape(
        rows_dev, top_k, width
    )
    shares = route_weights / jnp.sum(route_weights, axis=-1, keepdims=True)
    combined = jnp.sum(shares[:, :, None] * picked_rows.astype(jnp.float32), axis=1)
    return (wide + combined).astype(jnp.bfloat16)


def routing(meta, top_k, first, experts, capacity):
    rows = meta.shape[1]
    padded = max(experts, 16)
    expert = lax.broadcasted_iota(jnp.int32, (padded, rows), 0) + first
    expert = expert.astype(F32)
    weights = meta[top_k : 2 * top_k]
    total = jnp.sum(weights, axis=0, keepdims=True)
    member = jnp.zeros((padded, rows), F32)
    share = jnp.zeros((padded, rows), F32)
    for k in range(top_k):
        hit = jnp.where(meta[k : k + 1] == expert, 1.0, 0.0)
        member = member + hit
        share = share + hit * (weights[k : k + 1] / total)
    before = (
        lax.broadcasted_iota(jnp.int32, (rows, rows), 0)
        < lax.broadcasted_iota(jnp.int32, (rows, rows), 1)
    ).astype(BF16)
    rank = jnp.where(member > 0, dot(member.astype(BF16), before), -1.0)
    slots = experts * capacity
    spread = (
        lax.broadcasted_iota(jnp.int32, (slots, padded), 0) // capacity
        == lax.broadcasted_iota(jnp.int32, (slots, padded), 1)
    ).astype(BF16)
    place = lax.broadcasted_iota(jnp.int32, (slots, rows), 0) % capacity
    one = jnp.where(dot(spread, rank.astype(BF16)) == place.astype(F32), 1.0, 0.0)
    high = share.astype(BF16)
    low = (share - high.astype(F32)).astype(BF16)
    return (
        one.astype(BF16),
        (one * dot(spread, high)).astype(BF16),
        (one * dot(spread, low)).astype(BF16),
    )


def attend(sp_count, z, queries, kv, sink, halo, attended, send, recv):
    rows, lanes = kv.shape
    window = halo.shape[0]
    heads = sink.shape[1]
    size = queries.shape[1] // heads
    groups = lanes // (2 * size)
    share = heads // groups
    copy = pltpu.make_async_remote_copy(
        kv.at[pl.ds(rows - window, window)], halo, send, recv,
        device_id={"sp": jnp.minimum(z + 1, sp_count - 1)}, device_id_type=MESH,
    )

    @pl.when(z < sp_count - 1)
    def _():
        copy.start()

    pairs = share // 2
    tall = pairs * window
    query = lax.broadcasted_iota(jnp.int32, (tall, 2 * window), 0) % window
    key = lax.broadcasted_iota(jnp.int32, (tall, 2 * window), 1)
    distance = query + window - key
    band = (distance >= 0) & (distance < window)

    def block(b):
        allowed = band
        if b == 0:
            allowed = band & (z * rows - window + key >= 0)
            span = jnp.concatenate([halo[...], kv[:window]], 0)
        else:
            span = kv[(b - 1) * window : (b + 1) * window]
        here = slice(b * window, (b + 1) * window)
        for g in range(groups):
            keys = span[:, 2 * g * size : (2 * g + 1) * size]
            values = span[:, (2 * g + 1) * size : (2 * g + 2) * size]
            none, ones = jnp.zeros_like(keys), jnp.ones_like(values)
            wide = jnp.concatenate(
                [
                    queries[here, (g * share + 2 * i) * size : (g * share + 2 * i + 2) * size]
                    for i in range(pairs)
                ],
                0,
            )
            sides = []
            for odd in range(2):
                two_keys = jnp.concatenate([none, keys] if odd else [keys, none], 1)
                two_values = jnp.concatenate([ones, values] if odd else [values, ones], 1)
                score = dot(wide, two_keys, ((1,), (1,))) * size**-0.5
                score = jnp.where(allowed, score, -1e30)
                drain = jnp.concatenate(
                    [
                        jnp.broadcast_to(
                            sink[0:1, g * share + 2 * i + odd : g * share + 2 * i + odd + 1],
                            (window, 1),
                        )
                        for i in range(pairs)
                    ],
                    0,
                )
                top = jnp.maximum(jnp.max(score, axis=1, keepdims=True), drain)
                grown = jnp.exp(score - top).astype(BF16)
                both = dot(grown, two_values)
                at = 0 if odd else size
                total = both[:, at : at + 1] + jnp.exp(drain - top)
                sides.append(both * (1.0 / total))
            lane = lax.broadcasted_iota(jnp.int32, (tall, 2 * size), 1)
            both = jnp.where(lane < size, sides[0], sides[1]).astype(BF16)
            for i in range(pairs):
                first = (g * share + 2 * i) * size
                attended[here, first : first + 2 * size] = both[i * window : (i + 1) * window]

    for b in range(1, rows // window):
        block(b)

    @pl.when(z == 0)
    def _():
        halo[...] = jnp.zeros_like(halo)

    @pl.when(z > 0)
    def _():
        copy.wait_recv()

    block(0)

    @pl.when(z < sp_count - 1)
    def _():
        copy.wait_send()


def tail_kernel(
    sizes,
    queries, kv, sink, out_w_hbm, residual, gain, ids, weights, gate_hbm, up_hbm, down_hbm,
    out,
    halo, attended, halo_send, halo_recv,
    out_w, gate_w, up_w, down_w,
    pair_out, pair_in, far_out, far_in,
    load_sem, pair_send, pair_recv, far_send, far_recv,
    meta, meta_send, meta_recv,
    stream, picks, share_hi, share_lo,
    tokens, z_send, z_recv,
    sel_out, rows_in, a_send, a_recv,
    res_out, res_in, b_send, b_recv,
    held, part_out, from_low, from_high, r_send, low_recv, high_recv,
):
    sp_count, tp_count, pieces, capacity = sizes
    experts = sp_count * tp_count
    chips = tp_count // 2
    z, t = lax.axis_index("sp"), lax.axis_index("tp")
    me = z * tp_count + t
    x, core = t // 2, t % 2
    other = 1 - core
    rows, width = residual.shape
    piece = width // pieces

    def where(e):
        return {"sp": e // tp_count, "tp": e % tp_count}

    loads = [
        pltpu.make_async_copy(src, dst, load_sem.at[i])
        for i, (src, dst) in enumerate(
            ((out_w_hbm, out_w), (gate_hbm.at[0], gate_w), (up_hbm.at[0], up_w), (down_hbm.at[0], down_w))
        )
    ]
    for load in loads:
        load.start()

    barrier = pltpu.get_barrier_semaphore()

    def greet(k, carry):
        pl.semaphore_signal(
            barrier, inc=1, device_id=where((me + k) % experts), device_id_type=MESH
        )
        return carry

    lax.fori_loop(1, experts, greet, 0)
    top_k = ids.shape[0]
    meta[z, 0:top_k] = ids[...].astype(F32)
    meta[z, top_k : 2 * top_k] = weights[...]
    pl.semaphore_wait(barrier, experts - 1)

    def meta_copy(to, at):
        return pltpu.make_async_remote_copy(
            meta.at[at], meta.at[at], meta_send.at[to], meta_recv.at[at],
            device_id={"sp": to}, device_id_type=MESH,
        )

    for k in range(1, sp_count):
        meta_copy((z + k) % sp_count, z).start()
    attend(sp_count, z, queries, kv, sink, halo, attended, halo_send, halo_recv)
    loads[0].wait()

    def partial(chip, which, q):
        block = attended[pl.ds(pl.multiple_of((chip * 2 + which) * rows, rows), rows), :]
        return dot(block, out_w[:, q * piece : (q + 1) * piece])

    def pair_copy(k, q):
        return pltpu.make_async_remote_copy(
            pair_out.at[k, q], pair_in.at[k, q], pair_send.at[k, q], pair_recv.at[k, q],
            device_id={"tp": x * 2 + other}, device_id_type=MESH,
        )

    def far_copy(k, q):
        return pltpu.make_async_remote_copy(
            far_out.at[k, q], far_in.at[k, q], far_send.at[k, q], far_recv.at[k, q],
            device_id={"tp": ((x + k) % chips) * 2 + core}, device_id_type=MESH,
        )

    order = list(range(1, chips)) + [0]
    for q in range(pieces):
        for k in order:
            pair_out[k, q] = partial((x + k) % chips, other, q).astype(BF16)
            pair_copy(k, q).start()
        for k in range(1, chips):
            mine = partial((x + k) % chips, core, q)
            pair_copy(k, q).wait_recv()
            far_out[k, q] = (mine + pair_in[k, q].astype(F32)).astype(BF16)
            far_copy(k, q).start()
    for k in range(sp_count):
        j = (z + k) % sp_count
        if k:
            meta_copy(z, j).wait_recv()
        picks[j], share_hi[j], share_lo[j] = routing(
            meta[j], top_k, z * tp_count, tp_count, capacity
        )
    square = jnp.zeros((rows, 1), F32)
    for q in range(pieces):
        cols = slice(q * piece, (q + 1) * piece)
        total = partial(x, core, q)
        pair_copy(0, q).wait_recv()
        total = total + pair_in[0, q].astype(F32)
        for k in range(1, chips):
            far_copy(k, q).wait_recv()
            total = total + far_in[k, q].astype(F32)
        value = (residual[:, cols].astype(F32) + total).astype(BF16)
        stream[:, cols] = value
        value = value.astype(F32)
        square = square + jnp.sum(value * value, axis=1, keepdims=True)
    scale = lax.rsqrt(square / width + EPS)
    last = sp_count - 1
    above, below = jnp.minimum(z + 1, last), jnp.maximum(z - 1, 0)

    def z_copy(j, q, to, lane):
        return pltpu.make_async_remote_copy(
            tokens.at[j, q], tokens.at[j, q], z_send.at[lane, j, q], z_recv.at[j, q],
            device_id={"sp": to}, device_id_type=MESH,
        )

    def a_copy(j, q, to, at):
        return pltpu.make_async_remote_copy(
            sel_out.at[j, q, to], rows_in.at[j, q, at], a_send.at[j, q, to], a_recv.at[j, q, at],
            device_id={"tp": to}, device_id_type=MESH,
        )

    def b_copy(j, q, to, at):
        return pltpu.make_async_remote_copy(
            res_out.at[j, q, to], res_in.at[j, q, at], b_send.at[j, q, to], b_recv.at[j, q, at],
            device_id={"tp": to}, device_id_type=MESH,
        )

    def up_copy(j, q):
        return pltpu.make_async_remote_copy(
            part_out.at[j, q], from_low.at[j, q], r_send.at[j, q], low_recv.at[j, q],
            device_id={"sp": above}, device_id_type=MESH,
        )

    def down_copy(j, q):
        return pltpu.make_async_remote_copy(
            part_out.at[j, q], from_high.at[j, q], r_send.at[j, q], high_recv.at[j, q],
            device_id={"sp": below}, device_id_type=MESH,
        )

    for q in range(pieces):
        cols = slice(q * piece, (q + 1) * piece)
        tokens[z, q] = (stream[:, cols].astype(F32) * scale * gain[:, cols]).astype(BF16)

        @pl.when(z < last)
        def _():
            z_copy(z, q, above, 0).start()

        @pl.when(z > 0)
        def _():
            z_copy(z, q, below, 1).start()

    sign = 1 - 2 * ((2 * z) // sp_count)
    near = jnp.minimum(z, last - z)

    def nth(step):
        turn = (step + 1) // 2
        turn = z + sign * (turn if step % 2 else -turn)
        return jnp.where(2 * near >= step, turn, z + sign * (step - near))

    slots = tp_count * capacity
    peers = [(t + k) % tp_count for k in range(1, tp_count)]

    def choose(step):
        j = nth(step)
        for q in range(pieces):
            if step:
                z_copy(j, q, z, 0).wait_recv()

                @pl.when((j < z) & (z < last))
                def _():
                    z_copy(j, q, above, 0).start()

                @pl.when((j > z) & (z > 0))
                def _():
                    z_copy(j, q, below, 0).start()

            chosen = dot(picks[j], tokens[j, q]).astype(BF16)
            sel_out[j, q] = chosen.reshape(tp_count, capacity, piece)
            for i in peers:
                a_copy(j, q, i, t).start()
            rows_in[j, q, t] = sel_out[j, q, t]

    def expert(step):
        j = nth(step)
        hidden = gate_w.shape[1]
        gated = jnp.zeros((slots, hidden), F32)
        raised = jnp.zeros((slots, hidden), F32)
        for q in range(pieces):
            for i in peers:
                a_copy(j, q, t, i).wait_recv()
            block = rows_in[j, q].reshape(slots, piece)
            gated = gated + dot(block, gate_w[q * piece : (q + 1) * piece, :])
            raised = raised + dot(block, up_w[q * piece : (q + 1) * piece, :])
        active = (gated / (1.0 + jnp.exp(-gated)) * raised).astype(BF16)
        for q in range(pieces):
            done = dot(active, down_w[:, q * piece : (q + 1) * piece]).astype(BF16)
            res_out[j, q] = done.reshape(tp_count, capacity, piece)
            for i in peers:
                b_copy(j, q, i, t).start()
            res_in[j, q, t] = res_out[j, q, t]

    def blend(step):
        j = nth(step)
        for q in range(pieces):
            for i in peers:
                b_copy(j, q, t, i).wait_recv()
            block = res_in[j, q].reshape(slots, piece)
            total = dot(share_hi[j], block, ((0,), (0,))) + dot(share_lo[j], block, ((0,), (0,)))
            held[j, q] = total

            @pl.when((j < z) & (z == last))
            def _():
                part_out[j, q] = total.astype(BF16)
                down_copy(j, q).start()

            @pl.when((j > z) & (z == 0))
            def _():
                part_out[j, q] = total.astype(BF16)
                up_copy(j, q).start()

    for step in range(sp_count):
        choose(step)
        if step:
            blend(step - 1)
        else:
            for load in loads[1:]:
                load.wait()
        expert(step)
    blend(last)

    reach = [max(j, last - j) for j in range(sp_count)]
    for far in sorted(set(reach)):
        for q in range(pieces):
            cols = slice(q * piece, (q + 1) * piece)
            for j in [j for j in range(sp_count) if reach[j] == far]:

                @pl.when((z >= j) & (z < last))
                def _():
                    down_copy(j, q).wait_recv()
                    held[j, q] += from_high[j, q].astype(F32)

                @pl.when((z <= j) & (z > 0))
                def _():
                    up_copy(j, q).wait_recv()
                    held[j, q] += from_low[j, q].astype(F32)

                @pl.when((z > j) & (z < last))
                def _():
                    part_out[j, q] = held[j, q].astype(BF16)
                    down_copy(j, q).start()

                @pl.when((z < j) & (z > 0))
                def _():
                    part_out[j, q] = held[j, q].astype(BF16)
                    up_copy(j, q).start()

                @pl.when(z == j)
                def _():
                    out[:, cols] = (stream[:, cols].astype(F32) + held[j, q]).astype(BF16)

    for k in range(1, sp_count):
        meta_copy((z + k) % sp_count, z).wait_send()
    for q in range(pieces):
        for k in range(chips):
            pair_copy(k, q).wait_send()
            if k:
                far_copy(k, q).wait_send()

        @pl.when(z < last)
        def _():
            z_copy(z, q, above, 0).wait_send()

        @pl.when(z > 0)
        def _():
            z_copy(z, q, below, 1).wait_send()

        for k in range(sp_count):
            j = (z + k) % sp_count
            for i in peers:
                a_copy(j, q, i, t).wait_send()
                b_copy(j, q, i, t).wait_send()
            if k:
                up_copy(j, q).wait_send()

                @pl.when(((j < z) & (z < last)) | ((j > z) & (z > 0)))
                def _():
                    z_copy(j, q, above, 0).wait_send()


def fused(
    queries, key_heads, value_heads, sink_logit, out_weight, residual, norm_gain, expert_ids, route_weights,
    gate_weight, up_weight, down_weight,
):
    rows, width = residual.shape
    sp_count, tp_count = lax.axis_size("sp"), lax.axis_size("tp")
    experts = sp_count * tp_count
    top_k = expert_ids.shape[1]
    capacity = max(2, 2 * top_k * rows // experts)
    hidden = gate_weight.shape[2]
    depth = out_weight.shape[0]
    pieces = 4
    chips = tp_count // 2
    part = (chips, pieces, rows, width // pieces)
    blocks = (sp_count, pieces, rows, width // pieces)
    boxes = (sp_count, pieces, tp_count, capacity, width // pieces)
    seen, groups, size = key_heads.shape
    kv = jnp.stack([key_heads, value_heads], 2).reshape(seen, groups * 2 * size)
    vmem = pl.BlockSpec(memory_space=pltpu.VMEM)
    hbm = pl.BlockSpec(memory_space=pl.ANY)
    dma = pltpu.SemaphoreType.DMA
    return pl.pallas_call(
        functools.partial(tail_kernel, (sp_count, tp_count, pieces, capacity)),
        out_shape=jax.ShapeDtypeStruct((rows, width), BF16),
        in_specs=[vmem, vmem, vmem, hbm, vmem, vmem, vmem, vmem, hbm, hbm, hbm],
        out_specs=vmem,
        scratch_shapes=[
            pltpu.VMEM((WINDOW, kv.shape[1]), BF16),
            pltpu.VMEM(queries.shape, BF16),
            dma,
            dma,
            pltpu.VMEM((depth, width), BF16),
            pltpu.VMEM((width, hidden), BF16),
            pltpu.VMEM((width, hidden), BF16),
            pltpu.VMEM((hidden, width), BF16),
            pltpu.VMEM(part, BF16),
            pltpu.VMEM(part, BF16),
            pltpu.VMEM(part, BF16),
            pltpu.VMEM(part, BF16),
            dma((4,)),
            dma((chips, pieces)),
            dma((chips, pieces)),
            dma((chips, pieces)),
            dma((chips, pieces)),
            pltpu.VMEM((sp_count, -(-2 * top_k // 8) * 8, rows), F32),
            dma((sp_count,)),
            dma((sp_count,)),
            pltpu.VMEM((rows, width), BF16),
            *[pltpu.VMEM((sp_count, tp_count * capacity, rows), BF16)] * 3,
            pltpu.VMEM(blocks, BF16),
            dma((2, sp_count, pieces)),
            dma((sp_count, pieces)),
            *[pltpu.VMEM(boxes, BF16)] * 2,
            *[dma((sp_count, pieces, tp_count))] * 2,
            *[pltpu.VMEM(boxes, BF16)] * 2,
            *[dma((sp_count, pieces, tp_count))] * 2,
            pltpu.VMEM(blocks, F32),
            *[pltpu.VMEM(blocks, BF16)] * 3,
            *[dma((sp_count, pieces))] * 3,
        ],
        compiler_params=pltpu.CompilerParams(
            collective_id=0, has_side_effects=True, vmem_limit_bytes=VMEM_BUDGET
        ),
    )(
        queries, kv, sink_logit[None], out_weight, residual, norm_gain[None], expert_ids.T, route_weights.T,
        gate_weight, up_weight, down_weight,
    )


def on_device(queries, key_heads, value_heads, sink_logit, *rest):
    rows_dev = rest[1].shape[0]
    experts = lax.axis_size("sp") * lax.axis_size("tp")
    fits = 2 * rest[3].shape[1] * rows_dev // experts % 16 == 0
    if fits:
        return fused(queries, key_heads, value_heads, sink_logit, *rest)
    return tail_plain(attention(queries, key_heads, value_heads, sink_logit), *rest)


def solution(mesh):
    return jax.shard_map(
        on_device,
        mesh=mesh,
        in_specs=(
            P(("grp", "sp"), "tp"),
            P(("grp", "sp"), "tp", None),
            P(("grp", "sp"), "tp", None),
            P("tp"),
            P("tp", None),
            P(("grp", "sp", "tp"), None),
            P(),
            P(("grp", "sp", "tp"), None),
            P(("grp", "sp", "tp"), None),
            P(("sp", "tp"), None, None),
            P(("sp", "tp"), None, None),
            P(("sp", "tp"), None, None),
        ),
        out_specs=P(("grp", "sp", "tp"), None),
        check_vma=False,
    )
```

```python
import functools

import jax
import jax.numpy as jnp
from jax import lax
from jax.experimental import pallas as pl
from jax.experimental.pallas import tpu as pltpu
from jax.sharding import PartitionSpec as P

WINDOW = 128


EPS = 1e-06

F32 = jnp.float32
BF16 = jnp.bfloat16
MESH = pl.DeviceIdType.MESH
VMEM_BUDGET = 56 * 1024 * 1024


def from_behind(value, axis, steps):
    count = lax.axis_size(axis)
    initial, last = (max(0, -steps), min(count, count - steps))
    return lax.ppermute(value, axis, [(source, source + steps) for source in range(initial, last)])


def dot(a, b, dims=((1,), (0,))):
    return lax.dot_general(a, b, (dims, ((), ())), preferred_element_type=F32)


def attention(queries, key_heads, value_heads, sink_logit):
    rows_sp = queries.shape[0]
    kv_local = key_heads.shape[1]
    head_dim = key_heads.shape[2]
    heads_local = queries.shape[1] // head_dim
    group_size = heads_local // kv_local
    window = WINDOW
    count_of_blocks = rows_sp // window
    edge = jnp.stack([key_heads[rows_sp - window :], value_heads[rows_sp - window :]])
    tail_rows = from_behind(edge, "sp", 1)
    key_blocks = jnp.concatenate([tail_rows[0], key_heads], 0).reshape(
        count_of_blocks + 1, window, kv_local, head_dim
    )
    value_blocks = jnp.concatenate([tail_rows[1], value_heads], 0).reshape(
        count_of_blocks + 1, window, kv_local, head_dim
    )
    key_span = jnp.concatenate([key_blocks[:-1], key_blocks[1:]], 1)
    value_span = jnp.concatenate([value_blocks[:-1], value_blocks[1:]], 1)
    query_pos = jnp.arange(window, dtype=jnp.int32)[:, None]
    key_pos = jnp.arange(2 * window, dtype=jnp.int32)[None, :]
    distance = query_pos + window - key_pos
    band = (distance >= 0) & (distance < window)
    key_start = (
        lax.axis_index("sp") * rows_sp
        + jnp.arange(count_of_blocks, dtype=jnp.int32)[:, None] * window
        - window
        + key_pos
    )
    allowed = band[None, :, :] & (key_start >= 0)[:, None, :]
    query_blocks = queries.reshape(count_of_blocks, window, kv_local, group_size, head_dim)
    logit_scores = jnp.einsum(
        "bqhgd,bkhd->bhgqk", query_blocks, key_span, preferred_element_type=jnp.float32
    ) * head_dim ** (-0.5)
    logit_scores = jnp.where(allowed[:, None, None], logit_scores, -jnp.inf)
    sink_col = sink_logit.reshape(kv_local, group_size)[None, :, :, None, None]
    row_max = jnp.maximum(jnp.max(logit_scores, axis=-1, keepdims=True), sink_col)
    expd = jnp.exp(logit_scores - row_max)
    row_total = jnp.sum(expd, axis=-1, keepdims=True) + jnp.exp(sink_col - row_max)
    attention_probabilities = (expd / row_total).astype(jnp.bfloat16)
    attended = jnp.einsum(
        "bhgqk,bkhd->bqhgd", attention_probabilities, value_span, preferred_element_type=jnp.float32
    ).astype(jnp.bfloat16)
    return attended.reshape(rows_sp, heads_local * head_dim)


def tail_plain(
    attended, out_weight, residual, norm_gain, expert_ids, route_weights,
    gate_weight, up_weight, down_weight,
):
    rows_dev = residual.shape[0]
    width = residual.shape[1]
    projected = lax.psum_scatter(
        jnp.dot(attended, out_weight, preferred_element_type=jnp.float32),
        "tp",
        scatter_dimension=0,
        tiled=True,
    )
    stream = (residual.astype(jnp.float32) + projected).astype(jnp.bfloat16)
    wide = stream.astype(jnp.float32)
    normed = (
        wide * lax.rsqrt(jnp.mean(wide * wide, axis=-1, keepdims=True) + EPS) * norm_gain
    ).astype(jnp.bfloat16)
    sp_count = lax.axis_size("sp")
    tp_count = lax.axis_size("tp")
    experts_total = sp_count * tp_count
    top_k = expert_ids.shape[1]
    capacity = max(2, 2 * top_k * rows_dev // experts_total)
    flat_ids = expert_ids.reshape(-1)
    pairs = flat_ids.shape[0]
    onehot = (flat_ids[:, None] == jnp.arange(experts_total, dtype=jnp.int32)[None, :]).astype(
        jnp.int32
    )
    earlier = jnp.cumsum(onehot, axis=0) - onehot
    slot_rank = jnp.sum(earlier * onehot, axis=1)
    flat_slot = flat_ids * capacity + slot_rank
    owner_row = jnp.arange(pairs, dtype=jnp.int32) // top_k
    token_in_slot = jnp.zeros((experts_total * capacity,), jnp.int32).at[flat_slot].set(owner_row)
    filled = jnp.zeros((experts_total * capacity,), jnp.bool_).at[flat_slot].set(True)
    outbox = jnp.where(filled[:, None], normed[token_in_slot], jnp.zeros((), jnp.bfloat16))
    outbox = outbox.reshape(experts_total, capacity, width)
    arrived = lax.all_to_all(outbox, ("sp", "tp"), split_axis=0, concat_axis=0, tiled=True)
    rows = arrived.reshape(-1, width)
    gate = jnp.dot(rows, gate_weight[0], preferred_element_type=jnp.float32)
    upward = jnp.dot(rows, up_weight[0], preferred_element_type=jnp.float32)
    expert_hidden = (jax.nn.silu(gate) * upward).astype(jnp.bfloat16)
    expert_rows = jnp.dot(expert_hidden, down_weight[0], preferred_element_type=jnp.float32).astype(
        jnp.bfloat16
    )
    results = expert_rows.reshape(arrived.shape)
    returned = lax.all_to_all(results, ("sp", "tp"), split_axis=0, concat_axis=0, tiled=True)
    picked_rows = returned.reshape(experts_total * capacity, width)[flat_slot].reshape(
        rows_dev, top_k, width
    )
    shares = route_weights / jnp.sum(route_weights, axis=-1, keepdims=True)
    combined = jnp.sum(shares[:, :, None] * picked_rows.astype(jnp.float32), axis=1)
    return (wide + combined).astype(jnp.bfloat16)


def routing(ids, weights, experts, capacity):
    top_k, rows = ids.shape
    pad = jnp.zeros((-2 * top_k % 8, rows), F32)
    facts = jnp.concatenate([ids.astype(F32), weights, pad], 0).T
    ids, weights = facts[:, :top_k], facts[:, top_k : 2 * top_k]
    expert = lax.broadcasted_iota(jnp.int32, (rows, experts), 1).astype(F32)
    total = jnp.sum(weights, axis=1, keepdims=True)
    member = jnp.zeros((rows, experts), F32)
    share = jnp.zeros((rows, experts), F32)
    for k in range(top_k):
        hit = jnp.where(ids[:, k : k + 1] == expert, 1.0, 0.0)
        member = member + hit
        share = share + hit * (weights[:, k : k + 1] / total)
    before = (
        lax.broadcasted_iota(jnp.int32, (rows, rows), 0)
        > lax.broadcasted_iota(jnp.int32, (rows, rows), 1)
    ).astype(BF16)
    rank = dot(before, member.astype(BF16))
    rank = jnp.where(member > 0, rank, -1.0)
    slots = experts * capacity
    spread = (
        lax.broadcasted_iota(jnp.int32, (experts, slots), 1) // capacity
        == lax.broadcasted_iota(jnp.int32, (experts, slots), 0)
    ).astype(BF16)
    rank_slot = dot(rank.astype(BF16), spread)
    place = lax.broadcasted_iota(jnp.int32, (rows, slots), 1) % capacity
    taken = rank_slot == place.astype(F32)
    high = share.astype(BF16)
    low = (share - high.astype(F32)).astype(BF16)
    one = jnp.where(taken, 1.0, 0.0)
    return (
        one.astype(BF16),
        (one * dot(high, spread)).astype(BF16),
        (one * dot(low, spread)).astype(BF16),
    )


def attend(z, token_rows, queries, sink, seen, attended, at):
    window = WINDOW
    rows, lanes = queries.shape[0], seen.shape[1]
    heads = sink.shape[1]
    size = queries.shape[1] // heads
    groups = lanes // (2 * size)
    share = heads // groups
    pairs = share // 2
    tall = pairs * window
    query = lax.broadcasted_iota(jnp.int32, (tall, 2 * window), 0) % window
    key = lax.broadcasted_iota(jnp.int32, (tall, 2 * window), 1)
    distance = query + window - key
    band = (distance >= 0) & (distance < window)

    def block(b):
        allowed = band & ((z * rows + b * window - window) + key >= 0)
        span = seen[pl.ds(pl.multiple_of(b * window, window), 2 * window), :]
        here = pl.ds(pl.multiple_of(b * window, window), window)
        for g in range(groups):
            keys = span[:, 2 * g * size : (2 * g + 1) * size]
            values = span[:, (2 * g + 1) * size : (2 * g + 2) * size]
            none, ones = jnp.zeros_like(keys), jnp.ones_like(values)
            wide = jnp.concatenate(
                [
                    queries[here, (g * share + 2 * i) * size : (g * share + 2 * i + 2) * size]
                    for i in range(pairs)
                ],
                0,
            )
            sides = []
            for odd in range(2):
                two_keys = jnp.concatenate([none, keys] if odd else [keys, none], 1)
                two_values = jnp.concatenate([ones, values] if odd else [values, ones], 1)
                score = dot(wide, two_keys, ((1,), (1,))) * size**-0.5
                score = jnp.where(allowed, score, -1e30)
                drain = jnp.concatenate(
                    [
                        jnp.broadcast_to(
                            sink[0:1, g * share + 2 * i + odd : g * share + 2 * i + odd + 1],
                            (window, 1),
                        )
                        for i in range(pairs)
                    ],
                    0,
                )
                top = jnp.maximum(jnp.max(score, axis=1, keepdims=True), drain)
                grown = jnp.exp(score - top).astype(BF16)
                both = dot(grown, two_values)
                at = 0 if odd else size
                total = both[:, at : at + 1] + jnp.exp(drain - top)
                sides.append(both * (1.0 / total))
            lane = lax.broadcasted_iota(jnp.int32, (tall, 2 * size), 1)
            both = jnp.where(lane < size, sides[0], sides[1]).astype(BF16)
            for i in range(pairs):
                first = (g * share + 2 * i) * size
                attended[here, first : first + 2 * size] = both[i * window : (i + 1) * window]

    for b in range(token_rows // window):
        block(at * (token_rows // window) + b)


def tail_kernel(
    sizes,
    queries, kv, sink, out_w_hbm, residual, gain, ids, weights, gate_hbm, up_hbm, down_hbm,
    out,
    seen, attended, halo_send, halo_recv,
    out_w, gate_w, up_w, down_w,
    pair_out, pair_in, far_out, far_in,
    stream, normed, slots, share_hi, share_lo,
    outbox, arrived, results, returned,
    load_sem, pair_send, pair_recv, far_send, far_recv,
    go_send, go_recv, back_send, back_recv,
):
    sp_count, tp_count, pieces, capacity = sizes
    experts = sp_count * tp_count
    chips = tp_count // 2
    z, t = lax.axis_index("sp"), lax.axis_index("tp")
    me = z * tp_count + t
    x, core = t // 2, t % 2
    other = 1 - core
    rows, width = residual.shape
    piece = width // pieces

    def where(e):
        return {"sp": e // tp_count, "tp": e % tp_count}

    loads = [
        pltpu.make_async_copy(src, dst, load_sem.at[i])
        for i, (src, dst) in enumerate(
            ((out_w_hbm, out_w), (gate_hbm.at[0], gate_w), (up_hbm.at[0], up_w), (down_hbm.at[0], down_w))
        )
    ]
    for load in loads:
        load.start()

    barrier = pltpu.get_barrier_semaphore()

    def greet(k, carry):
        pl.semaphore_signal(
            barrier, inc=1, device_id=where((me + k) % experts), device_id_type=MESH
        )
        return carry

    lax.fori_loop(1, experts, greet, 0)
    pl.semaphore_wait(barrier, experts - 1)
    reach = kv.shape[0]
    halo_copy = pltpu.make_async_remote_copy(
        kv.at[pl.ds(reach - WINDOW, WINDOW)], seen.at[pl.ds(0, WINDOW)], halo_send, halo_recv,
        device_id={"sp": jnp.minimum(z + 1, sp_count - 1)}, device_id_type=MESH,
    )

    @pl.when(z < sp_count - 1)
    def _():
        halo_copy.start()

    seen[WINDOW:, :] = kv[...]
    slots[...], share_hi[...], share_lo[...] = routing(ids[...], weights[...], experts, capacity)

    @pl.when(z == 0)
    def _():
        seen[:WINDOW, :] = jnp.zeros((WINDOW, kv.shape[1]), BF16)

    @pl.when(z > 0)
    def _():
        halo_copy.wait_recv()

    loads[0].wait()

    def partial(chip, which, q):
        block = attended[pl.ds(pl.multiple_of((chip * 2 + which) * rows, rows), rows), :]
        return dot(block, out_w[:, q * piece : (q + 1) * piece])

    def pair_copy(k, q):
        return pltpu.make_async_remote_copy(
            pair_out.at[k, q], pair_in.at[k, q], pair_send.at[k, q], pair_recv.at[k, q],
            device_id={"tp": x * 2 + other}, device_id_type=MESH,
        )

    def far_copy(k, q):
        return pltpu.make_async_remote_copy(
            far_out.at[k, q], far_in.at[k, q], far_send.at[k, q], far_recv.at[k, q],
            device_id={"tp": ((x + k) % chips) * 2 + core}, device_id_type=MESH,
        )

    order = list(range(1, chips)) + [0]
    for k in order:
        chip = (x + k) % chips
        attend(z, rows, queries, sink, seen, attended, chip * 2 + other)
        for q in range(pieces):
            pair_out[k, q] = partial(chip, other, q).astype(BF16)
            pair_copy(k, q).start()
        attend(z, rows, queries, sink, seen, attended, chip * 2 + core)
        for q in range(pieces if k else 0):
            mine = partial(chip, core, q)
            pair_copy(k, q).wait_recv()
            far_out[k, q] = (mine + pair_in[k, q].astype(F32)).astype(BF16)
            far_copy(k, q).start()
    square = jnp.zeros((rows, 1), F32)
    for q in range(pieces):
        cols = slice(q * piece, (q + 1) * piece)
        total = partial(x, core, q)
        pair_copy(0, q).wait_recv()
        total = total + pair_in[0, q].astype(F32)
        for k in range(1, chips):
            far_copy(k, q).wait_recv()
            total = total + far_in[k, q].astype(F32)
        value = (residual[:, cols].astype(F32) + total).astype(BF16)
        stream[:, cols] = value
        value = value.astype(F32)
        square = square + jnp.sum(value * value, axis=1, keepdims=True)
    scale = lax.rsqrt(square / width + EPS)
    for q in range(pieces):
        cols = slice(q * piece, (q + 1) * piece)
        normed[:, cols] = (stream[:, cols].astype(F32) * scale * gain[:, cols]).astype(BF16)

    def go_copy(to, at):
        return pltpu.make_async_remote_copy(
            outbox.at[to], arrived.at[at], go_send.at[to], go_recv.at[at],
            device_id=where(to), device_id_type=MESH,
        )

    def back_copy(to, at):
        return pltpu.make_async_remote_copy(
            results.at[to], returned.at[at], back_send.at[to], back_recv.at[at],
            device_id=where(to), device_id_type=MESH,
        )

    picks = tp_count * capacity
    for d in range(sp_count):
        layer = range(d * tp_count, (d + 1) * tp_count)
        chosen = dot(slots[:, d * picks : (d + 1) * picks], normed[...], ((0,), (0,))).astype(BF16)
        for i, e in enumerate(layer):
            outbox[e] = chosen[i * capacity : (i + 1) * capacity]

            @pl.when(e != me)
            def _():
                go_copy(e, me).start()

    arrived[me] = outbox[me]
    for load in loads[1:]:
        load.wait()

    def expert(d, carry):
        layer = (z + d) % sp_count
        for i in range(tp_count):
            e = layer * tp_count + i

            @pl.when(e != me)
            def _():
                go_copy(me, e).wait_recv()

        block = arrived[pl.ds(layer * tp_count, tp_count)].reshape(picks, width)
        gated = dot(block, gate_w[...])
        raised = dot(block, up_w[...])
        hidden = (gated / (1.0 + jnp.exp(-gated)) * raised).astype(BF16)
        done = dot(hidden, down_w[...]).astype(BF16)
        results[pl.ds(layer * tp_count, tp_count)] = done.reshape(tp_count, capacity, width)
        for i in range(tp_count):
            e = layer * tp_count + i

            @pl.when(e != me)
            def _():
                back_copy(e, me).start()

        return carry

    lax.fori_loop(0, sp_count, expert, 0)
    returned[me] = results[me]

    def collect(k, carry):
        e = (me + k) % experts
        back_copy(me, e).wait_recv()
        return carry

    lax.fori_loop(1, experts, collect, 0)
    for q in range(pieces):
        cols = slice(q * piece, (q + 1) * piece)
        back = returned[:, :, cols].reshape(experts * capacity, piece)
        mixed = dot(share_hi[...], back) + dot(share_lo[...], back)
        out[:, cols] = (stream[:, cols].astype(F32) + mixed).astype(BF16)

    @pl.when(z < sp_count - 1)
    def _():
        halo_copy.wait_send()

    for q in range(pieces):
        for k in range(chips):
            pair_copy(k, q).wait_send()
            if k:
                far_copy(k, q).wait_send()

    def flush(k, carry):
        e = (me + k) % experts
        go_copy(e, me).wait_send()
        back_copy(e, me).wait_send()
        return carry

    lax.fori_loop(1, experts, flush, 0)


def fused(
    queries, key_heads, value_heads, sink_logit, out_weight, residual, norm_gain, expert_ids, route_weights,
    gate_weight, up_weight, down_weight,
):
    rows, width = residual.shape
    sp_count, tp_count = lax.axis_size("sp"), lax.axis_size("tp")
    experts = sp_count * tp_count
    top_k = expert_ids.shape[1]
    capacity = max(2, 2 * top_k * rows // experts)
    hidden = gate_weight.shape[2]
    depth = out_weight.shape[0]
    pieces = 4
    chips = tp_count // 2
    part = (chips, pieces, rows, width // pieces)
    box = (experts, capacity, width)
    reach, groups, size = key_heads.shape
    kv = jnp.stack([key_heads, value_heads], 2).reshape(reach, groups * 2 * size)
    vmem = pl.BlockSpec(memory_space=pltpu.VMEM)
    hbm = pl.BlockSpec(memory_space=pl.ANY)
    dma = pltpu.SemaphoreType.DMA
    return pl.pallas_call(
        functools.partial(tail_kernel, (sp_count, tp_count, pieces, capacity)),
        out_shape=jax.ShapeDtypeStruct((rows, width), BF16),
        in_specs=[vmem, vmem, vmem, hbm, vmem, vmem, vmem, vmem, hbm, hbm, hbm],
        out_specs=vmem,
        scratch_shapes=[
            pltpu.VMEM((WINDOW + kv.shape[0], kv.shape[1]), BF16),
            pltpu.VMEM(queries.shape, BF16),
            dma,
            dma,
            pltpu.VMEM((depth, width), BF16),
            pltpu.VMEM((width, hidden), BF16),
            pltpu.VMEM((width, hidden), BF16),
            pltpu.VMEM((hidden, width), BF16),
            pltpu.VMEM(part, BF16),
            pltpu.VMEM(part, BF16),
            pltpu.VMEM(part, BF16),
            pltpu.VMEM(part, BF16),
            pltpu.VMEM((rows, width), BF16),
            pltpu.VMEM((rows, width), BF16),
            pltpu.VMEM((rows, experts * capacity), BF16),
            pltpu.VMEM((rows, experts * capacity), BF16),
            pltpu.VMEM((rows, experts * capacity), BF16),
            pltpu.VMEM(box, BF16),
            pltpu.VMEM(box, BF16),
            pltpu.VMEM(box, BF16),
            pltpu.VMEM(box, BF16),
            dma((4,)),
            dma((chips, pieces)),
            dma((chips, pieces)),
            dma((chips, pieces)),
            dma((chips, pieces)),
            dma((experts,)),
            dma((experts,)),
            dma((experts,)),
            dma((experts,)),
        ],
        compiler_params=pltpu.CompilerParams(
            collective_id=0, has_side_effects=True, vmem_limit_bytes=VMEM_BUDGET
        ),
    )(
        queries, kv, sink_logit[None], out_weight, residual, norm_gain[None], expert_ids.T, route_weights.T,
        gate_weight, up_weight, down_weight,
    )


def on_device(queries, key_heads, value_heads, sink_logit, *rest):
    rows_dev = rest[1].shape[0]
    experts = lax.axis_size("sp") * lax.axis_size("tp")
    fits = 2 * rest[3].shape[1] * rows_dev // experts % 16 == 0 and rows_dev % WINDOW == 0
    if fits:
        return fused(queries, key_heads, value_heads, sink_logit, *rest)
    return tail_plain(attention(queries, key_heads, value_heads, sink_logit), *rest)


def solution(mesh):
    return jax.shard_map(
        on_device,
        mesh=mesh,
        in_specs=(
            P(("grp", "sp"), "tp"),
            P(("grp", "sp"), "tp", None),
            P(("grp", "sp"), "tp", None),
            P("tp"),
            P("tp", None),
            P(("grp", "sp", "tp"), None),
            P(),
            P(("grp", "sp", "tp"), None),
            P(("grp", "sp", "tp"), None),
            P(("sp", "tp"), None, None),
            P(("sp", "tp"), None, None),
            P(("sp", "tp"), None, None),
        ),
        out_specs=P(("grp", "sp", "tp"), None),
        check_vma=False,
    )
```
